256 devices in a mesh: sp: 32 (over z, y), tp: 8 (over x, core).
Axes of the slice: x: 4, y: 4, z: 8, core: 2. Of those that a mesh axis runs over, the one named last changes fastest.
Arguments:
- stream: bfloat16 [32768, 2048], P(('sp', 'tp')), may hold values from -6 to 6
- query_rows: bfloat16 [32768, 1024], P('sp', 'tp'), may hold values from -6 to 6
- key_rows: bfloat16 [32768, 1024], P('sp', 'tp'), may hold values from -6 to 6
- value_rows: bfloat16 [32768, 2048], P('sp', 'tp'), may hold values from -6 to 6
- gate_rows: bfloat16 [32768, 2048], P('sp', 'tp'), may hold values from -6 to 6
- log_decay: float32 [32768, 1024], P('sp', 'tp'), may hold values from -1 to 0
- head_gain: float32 [256], replicated, may hold values from 0.1 to 1.9
- out_weight: bfloat16 [2048, 2048], P('tp'), may hold values from -0.125 to 0.125
- mix_gain: float32 [2048], replicated, may hold values from 0.1 to 1.9
- up_weight: bfloat16 [2048, 8192], P('sp', 'tp'), may hold values from -0.125 to 0.125
- down_weight: bfloat16 [2048, 8192], P('sp', 'tp'), may hold values from -0.0625 to 0.0625
Outputs:
- mixed_out: bfloat16 [32768, 2048], P(('sp', 'tp'))
The draws below stay inside these ranges and needn't reach their ends.
All inputs are finite; a program needn't handle non-finite values.
Results may differ from the reference program's by a relative error of at most 0.02.
Values may be sent and summed in bfloat16 or wider, within the bound.
A program may use at most 128 MiB of HBM per device.

```python
import jax
import jax.numpy as jnp
from jax import lax

D = 2048
HEADS = 8
KEY_CHANNELS = 128
DV = 256
FF = 8192
BLOCK = 64
TOK_DEV = 1024
TOKENS = 32768
N_TP = 8


def draw_log_decay(key, part):
    keys = jax.random.split(jax.random.fold_in(key, 7), 7)
    devices = TOKENS // TOK_DEV
    width = HEADS * KEY_CHANNELS
    fast_share = 0.5
    noise = jax.random.uniform(keys[4], (TOKENS, width), jnp.float32, 0.5, 1.5)
    fast_head = jax.random.uniform(keys[0], (HEADS,), jnp.float32) < fast_share
    fast_channel = jnp.repeat(fast_head, KEY_CHANNELS)
    slow_rate = jnp.exp(jax.random.uniform(keys[1], (width,), jnp.float32, jnp.log(0.1), jnp.log(0.5))) / TOKENS
    fast_rate = jnp.exp(jax.random.uniform(keys[2], (width,), jnp.float32, jnp.log(0.02), jnp.log(0.033)))
    base = jnp.where(fast_channel, fast_rate, slow_rate)
    device_factor = jnp.exp(jax.random.uniform(keys[3], (devices, HEADS), jnp.float32, jnp.log(0.5), jnp.log(2.0)))
    device_rows = jnp.repeat(jnp.repeat(device_factor, TOK_DEV, axis=0), KEY_CHANNELS, axis=1)
    decay_rates = base[None, :] * device_rows * noise
    spots = jax.random.randint(keys[5], (2,), 0, TOKENS)
    decay_losses = jax.random.uniform(keys[6], (2, HEADS), jnp.float32, 0.2, 0.4)
    block_hits = (jnp.arange(TOKENS)[:, None] == spots[None, :]).astype(jnp.float32)
    block_surge = jnp.dot(block_hits, jnp.log(1.0 - decay_losses))
    return (jnp.repeat(block_surge, KEY_CHANNELS, axis=1) - decay_rates).astype(jnp.float32)


def shard_levels(own_key, shape, shards, smallest, largest):
    level = 1.0
    for dim, blocks in shards:
        steps = jax.random.uniform(jax.random.fold_in(jax.random.fold_in(own_key, 6), dim), (blocks,), jnp.float32, smallest / len(shards), largest / len(shards))
        level = level * jnp.repeat(jnp.exp(steps), shape[dim] // blocks).reshape((-1,) + (1,) * (len(shape) - 1 - dim))
    return level


def centred(rng, extent, scale, most, pieces=(), held_as=jnp.bfloat16):
    result = scale * jax.random.normal(rng, extent, jnp.float32)
    if pieces:
        result = result * shard_levels(rng, extent, pieces, -0.22, 0.18)
    return jnp.clip(result, -most, most).astype(held_as)


def setup_inputs(seed: int = 0) -> dict:
    key_of = jax.random.split(jax.random.key(seed), 12)
    stream = centred(key_of[0], (TOKENS, D), 1.0, 6.0, ((0, 256),))
    query_rows = centred(key_of[1], (TOKENS, HEADS * KEY_CHANNELS), 1.0, 6.0, ((0, 32), (1, 8)))
    key_rows = centred(key_of[2], (TOKENS, HEADS * KEY_CHANNELS), 1.0, 6.0, ((0, 32), (1, 8)))
    value_rows = centred(key_of[3], (TOKENS, HEADS * DV), 1.0, 6.0, ((0, 32), (1, 8)))
    gate_rows = centred(key_of[4], (TOKENS, HEADS * DV), 1.0, 6.0, ((0, 32), (1, 8)))
    log_decay = draw_log_decay(jax.random.fold_in(key_of[11], 71), 0)
    head_gain = jnp.clip(1.0 + 0.18 * jax.random.normal(key_of[6], (DV,), jnp.float32), 0.1, 1.9)
    out_weight = centred(key_of[7], (HEADS * DV, D), (HEADS * DV) ** -0.5, 0.125, ((0, 8),))
    mix_gain = jnp.clip(1.0 + 0.18 * jax.random.normal(key_of[8], (D,), jnp.float32), 0.1, 1.9)
    up_weight = centred(key_of[9], (D, FF), D ** -0.5, 0.125, ((0, 32), (1, 8)))
    down_weight = centred(key_of[10], (D, FF), FF ** -0.5, 0.0625, ((0, 32), (1, 8)))
    return {"stream": stream, "query_rows": query_rows, "key_rows": key_rows, "value_rows": value_rows, "gate_rows": gate_rows, "log_decay": log_decay, "head_gain": head_gain, "out_weight": out_weight, "mix_gain": mix_gain, "up_weight": up_weight, "down_weight": down_weight}


EPS = 1e-06

def attention(query_rows, key_rows, value_rows, log_decay):
    count = TOKENS // BLOCK
    queries = query_rows.astype(jnp.float32).reshape(count, BLOCK, HEADS, KEY_CHANNELS) * KEY_CHANNELS ** (-0.5)
    keys_all = key_rows.astype(jnp.float32).reshape(count, BLOCK, HEADS, KEY_CHANNELS)
    values_all = value_rows.astype(jnp.float32).reshape(count, BLOCK, HEADS, DV)
    decay_rates = log_decay.astype(jnp.float32).reshape(count, BLOCK, HEADS, KEY_CHANNELS)

    def step(matrix_state, inputs):
        query_block, kee, value_block, rate = inputs
        cum = jnp.cumsum(rate, axis=0)
        last = cum[-1:]
        decayed_state = kee * jnp.exp(last - cum)
        state_update = jnp.einsum('qzx,qzf->zxf', decayed_state, value_block, precision=lax.Precision.HIGHEST)
        matrix_state = jnp.exp(last[0])[..., None] * matrix_state + state_update
        head_output = jnp.einsum('wle,leg->wlg', query_block, matrix_state, precision=lax.Precision.HIGHEST)
        return (matrix_state, head_output)
    start = jnp.zeros((HEADS, KEY_CHANNELS, DV), jnp.float32)
    _, outs = lax.scan(step, start, (queries, keys_all, values_all, decay_rates))
    return outs.reshape(TOKENS, HEADS, DV)

def feed_block(rows_in, up_weight, down_weight):
    pre = jnp.dot(rows_in, up_weight, preferred_element_type=jnp.float32)
    hidden = jnp.square(jax.nn.relu(pre)).astype(jnp.bfloat16)
    group = FF // N_TP
    grouped = hidden.astype(jnp.float32).reshape(rows_in.shape[0], N_TP, group)
    downs = down_weight.astype(jnp.float32).reshape(D, N_TP, group)
    parts = jnp.einsum('rjf,djf->jrd', grouped, downs)
    parts = lax.optimization_barrier(parts.astype(jnp.bfloat16)).astype(jnp.float32)
    return lax.optimization_barrier(jnp.sum(parts, axis=0))

def reference(stream, query_rows, key_rows, value_rows, gate_rows, log_decay, head_gain, out_weight, mix_gain, up_weight, down_weight):
    readout = attention(query_rows, key_rows, value_rows, log_decay)
    scaled = readout * lax.rsqrt(lax.optimization_barrier(jnp.mean(readout * readout, axis=-1, keepdims=True)) + EPS)
    gates = gate_rows.astype(jnp.float32).reshape(TOKENS, HEADS, DV)
    gated = scaled * head_gain.astype(jnp.float32) * jax.nn.silu(gates)
    heads_out = gated.reshape(TOKENS, HEADS * DV).astype(jnp.bfloat16)
    attn = jnp.dot(heads_out, out_weight, preferred_element_type=jnp.float32)
    mid = (stream.astype(jnp.float32) + attn).astype(jnp.bfloat16)
    midf = mid.astype(jnp.float32)
    normed = (midf * lax.rsqrt(lax.optimization_barrier(jnp.mean(midf * midf, axis=-1, keepdims=True)) + EPS) * mix_gain.astype(jnp.float32)).astype(jnp.bfloat16)
    blocks = normed.reshape(TOKENS // TOK_DEV, TOK_DEV, D)
    feed = lax.map(lambda rows_in: feed_block(rows_in, up_weight, down_weight), blocks).reshape(TOKENS, D)
    return (midf + feed).astype(jnp.bfloat16)
```

```python
import functools

import jax
import jax.numpy as jnp
from jax import lax
from jax.experimental import pallas as pl
from jax.experimental.pallas import tpu as pltpu
from jax.sharding import Mesh
from jax.sharding import PartitionSpec as P

KC = 128
DV = 256
BLOCK = 64
D = 2048
ROWS = 1024
OWN = 128
NB = ROWS // BLOCK
NZ, NY, NX = 8, 4, 4
NSP = NZ * NY
Q = 2
QR = OWN // Q
HID = 1024
WR = 64
EPS = 1e-06
SP = ("sp_0", "sp_1")
TP = ("tp_0", "tp_1")
SP_TP = ("sp_0", "sp_1", "tp_0", "tp_1")
MESH = pl.DeviceIdType.MESH
F32 = jnp.float32
BF16 = jnp.bfloat16

_IDS = {}


def _id(name):
    return _IDS.setdefault(name, len(_IDS))


for _d in range(2):
    _id(("ay", _d))
    _id(("ayh", _d))
    for _i in (1, 2, 3, 4):
        _id(("bz", _d, _i))
        for _h in range(2):
            _id(("az", _d, _i, _h))
    for _k in range(8):
        _id(("by", _d, _k))
        _id(("byh", _d, _k))
    for _q in range(Q):
        for _rs in range(2):
            for _j in range(4):
                _id(("dd", _rs, _j, _q))
            for _s in (1, 2):
                _id(("rx", _rs, _s, _d, _q))
        _id(("ag", _d, _q))
        _id(("agh", _d, _q))
        for _j in range(4):
            _id(("ags", _j, _q))
_id("st1")
_id("st2")
N_IDS = len(_IDS)


def _dot(a, b, dims=(((1,), (0,)), ((), ()))):
    return lax.dot_general(a, b, dims, preferred_element_type=F32)


def _split(x):
    hi = x.astype(BF16)
    return hi, (x - hi.astype(F32)).astype(BF16)


def kernel(
    stream_h,
    q_h,
    k_h,
    v_h,
    g_h,
    ld_h,
    hg_ref,
    ow_h,
    mg_ref,
    up_h,
    dn_h,
    out_ref,
    stream_v,
    q_v,
    k_v,
    v_v,
    g_v,
    ld_v,
    ow_v,
    wu,
    wd,
    sloc,
    cl,
    sx_send,
    sx_recv,
    px_send,
    px_recv,
    psend,
    precv,
    pown,
    cs,
    r1,
    r2,
    nrm,
    mid_v,
    hid_v,
    lsem,
    ssem,
    rsem,
):
    z, y = lax.axis_index("sp_0"), lax.axis_index("sp_1")
    x, c = lax.axis_index("tp_0"), lax.axis_index("tp_1")
    sp = z * NY + y
    yl, yr = lax.rem(y + NY - 1, NY), lax.rem(y + 1, NY)
    zl, zr = lax.rem(z + NZ - 1, NZ), lax.rem(z + 1, NZ)
    xl, xr = lax.rem(x + NX - 1, NX), lax.rem(x + 1, NX)
    y_to, y_from = ({"sp_1": yr}, {"sp_1": yl}), (yl, yr)
    z_to = ({"sp_0": zr}, {"sp_0": zl})
    x_to = ({"tp_0": xr}, {"tp_0": xl})
    sib = {"tp_1": 1 - c}

    barrier = pltpu.get_barrier_semaphore()

    def greet(d, carry):
        t = lax.rem(sp + d, NSP)
        pl.semaphore_signal(
            barrier, inc=1, device_id={"sp_0": t // NY, "sp_1": lax.rem(t, NY)}, device_id_type=MESH
        )
        return carry

    loads = {}

    def load(name, src, dst, i):
        loads[name] = pltpu.make_async_copy(src, dst, lsem.at[i])
        loads[name].start()

    load("ld", ld_h, ld_v, 0)
    load("k", k_h, k_v, 1)
    load("v", v_h, v_v, 2)
    load("up", up_h, wu.at[sp], 3)
    load("dn", dn_h, wd.at[sp], 4)
    load("q", q_h, q_v, 5)
    load("g", g_h, g_v, 6)
    load("ow", ow_h, ow_v, 7)
    load("stream", stream_h, stream_v, 8)

    lax.fori_loop(1, NSP, greet, 0)
    for other in (x_to[0], x_to[1], sib):
        pl.semaphore_signal(barrier, inc=1, device_id=other, device_id_type=MESH)
    pl.semaphore_wait(barrier, NSP - 1 + 3)

    copies = {}

    def send(name, src, dst, to):
        i = _IDS[name]
        copies[name] = pltpu.make_async_remote_copy(
            src_ref=src,
            dst_ref=dst,
            send_sem=ssem.at[i],
            recv_sem=rsem.at[i],
            device_id=to,
            device_id_type=MESH,
        )
        copies[name].start()

    def arrived(name):
        copies[name].wait_recv()

    HALF = (pl.ds(0, WR // 2), pl.ds(WR // 2, WR // 2))

    def zat(off):
        return lax.rem(z + off + NZ, NZ)

    def up_slab(zz, h):
        return wu.at[pl.ds(zz * NY, NY), HALF[h]]

    def up_y():
        for d in range(2):
            send(("ay", d), wu.at[sp], wu.at[sp], y_to[d])

    def up_y_half():
        for d in range(2):
            arrived(("ay", d))
            part = wu.at[z * NY + y_from[d], HALF[d]]
            send(("ayh", d), part, part, y_to[d])

    def up_z(i):
        if i == 1:
            for d in range(2):
                arrived(("ayh", d))
        for h in range(2):
            for d in range(2):
                if i > 1:
                    arrived(("az", d, i - 1, h))
                if i == 4 and h != d:
                    continue
                part = up_slab(zat(-(i - 1) if d == 0 else i - 1), h)
                send(("az", d, i, h), part, part, z_to[d])

    def up_done():
        for d in range(2):
            arrived(("az", d, 4, d))

    def dn_z(i):
        for d in range(2):
            if i > 1:
                arrived(("bz", d, i - 1))
            blk = zat(-(i - 1) if d == 0 else i - 1) * NY + y
            part = wd.at[blk] if i < 4 else wd.at[blk, HALF[d]]
            send(("bz", d, i), part, part, z_to[d])

    def dn_z_done():
        for d in range(2):
            arrived(("bz", d, 4))

    def dn_y(k):
        part = wd.at[zat(k) * NY + y]
        for d in range(2):
            send(("by", d, k), part, part, y_to[d])

    def dn_y_half(k):
        for d in range(2):
            arrived(("by", d, k))
            part = wd.at[zat(k) * NY + y_from[d], HALF[d]]
            send(("byh", d, k), part, part, y_to[d])

    def dn_done():
        for k in range(8):
            for d in range(2):
                arrived(("byh", d, k))

    loads["up"].wait()
    loads["dn"].wait()
    dn_z(1)
    up_y()
    dn_y(0)

    loads["ld"].wait()
    loads["k"].wait()
    loads["v"].wait()
    r_i = lax.broadcasted_iota(jnp.int32, (256, 256), 0)
    c_i = lax.broadcasted_iota(jnp.int32, (256, 256), 1)
    tri = jnp.where((c_i > r_i) & (c_i // BLOCK == r_i // BLOCK), 1.0, 0.0).astype(BF16)

    def group(gi, carry):
        state, total = carry
        rows = pl.ds(pl.multiple_of(gi * 256, 256), 256)
        ld = ld_v[rows, :]
        hi, lo = _split(ld)
        lo2 = (ld - hi.astype(F32) - lo.astype(F32)).astype(BF16)
        suf = _dot(tri, hi) + _dot(tri, lo) + _dot(tri, lo2)
        dk = k_v[rows, :].astype(F32) * jnp.exp(suf)
        dk_hi, dk_lo = _split(dk)
        vals = v_v[rows, :]
        for b in range(4):
            s = slice(b * BLOCK, (b + 1) * BLOCK)
            vv = jnp.concatenate([vals[s], vals[s]], axis=0)
            dd = jnp.concatenate([dk_hi[s], dk_lo[s]], axis=0)
            upd = _dot(vv, dd, (((0,), (0,)), ((), ())))
            last = suf[b * BLOCK : b * BLOCK + 1] + ld[b * BLOCK : b * BLOCK + 1]
            state = jnp.exp(last) * state + upd
            total = total + last
            sloc[gi * 4 + b] = state
            cl[gi * 4 + b] = jnp.broadcast_to(total, (8, KC))
        return state, total

    state, total = lax.fori_loop(
        0, NB // 4, group, (jnp.zeros((DV, KC), F32), jnp.zeros((1, KC), F32))
    )

    t_hi, t_lo = _split(total)
    t_lo2 = (total - t_hi.astype(F32) - t_lo.astype(F32)).astype(BF16)
    sub = lax.broadcasted_iota(jnp.int32, (8, KC), 0)
    logs = jnp.where(
        sub == 0,
        t_hi.astype(F32),
        jnp.where(sub == 1, t_lo.astype(F32), jnp.where(sub == 2, t_lo2.astype(F32), 0.0)),
    )
    tiles = jnp.concatenate(
        [state.reshape(NSP, 8, KC), jnp.broadcast_to(logs[None], (NSP, 8, KC))], axis=1
    ).astype(BF16)
    sx_send[...] = tiles

    def all_of(dst, name, sem):
        part = dst.at[pl.ds(0, NSP - 1)]
        return pltpu.make_async_copy(part, part, sem.at[_IDS[name]])

    def scatter(src, dst, name):
        i = _IDS[name]

        def one(d, carry):
            t = lax.rem(sp + d, NSP)
            pltpu.make_async_remote_copy(
                src_ref=src.at[t],
                dst_ref=dst.at[sp],
                send_sem=ssem.at[i],
                recv_sem=rsem.at[i],
                device_id={"sp_0": t // NY, "sp_1": lax.rem(t, NY)},
                device_id_type=MESH,
            ).start()
            return carry

        lax.fori_loop(1, NSP, one, 0)
        dst[sp] = src[sp]

    scatter(sx_send, sx_recv, "st1")

    up_y_half()
    dn_z(2)
    dn_y(1)
    dn_y(7)

    all_of(sx_recv, "st1", rsem).wait()

    def prefix(e, run):
        px_send[e] = run
        tile = sx_recv[e].astype(F32)
        log = tile[8:9] + tile[9:10] + tile[10:11]
        return jnp.exp(log) * run + tile[0:8]

    lax.fori_loop(0, NSP, prefix, jnp.zeros((8, KC), F32))
    scatter(px_send, px_recv, "st2")

    dn_y_half(0)
    up_z(1)
    dn_z(3)
    dn_y(2)
    dn_y(6)

    loads["q"].wait()
    loads["g"].wait()
    loads["ow"].wait()
    all_of(px_recv, "st2", rsem).wait()

    def attend(j):
        s_in = px_recv[...].reshape(DV, KC)
        base = lax.rem(x + j, NX) * 4
        gain = hg_ref[...]
        outs = []
        for half in range(2):
            first = base + (1 - c if half == 0 else c) * 2
            for b in range(2):
                n = first + b
                rows = pl.ds(pl.multiple_of(n * BLOCK, BLOCK), BLOCK)
                full = sloc[n] + jnp.exp(cl[n][0:1]) * s_in
                f_hi, f_lo = _split(full)
                qq = q_v[rows, :]
                read = _dot(
                    jnp.concatenate([qq, qq], axis=1),
                    jnp.concatenate([f_hi, f_lo], axis=1),
                    (((1,), (1,)), ((), ())),
                ) * (KC**-0.5)
                scaled = read * lax.rsqrt(jnp.mean(read * read, axis=-1, keepdims=True) + EPS)
                gate = g_v[rows, :].astype(F32)
                outs.append((scaled * gain * (gate / (1.0 + jnp.exp(-gate)))).astype(BF16))
        heads = jnp.concatenate(outs, axis=0)
        for n in range(4):
            cols = slice(n * 512, (n + 1) * 512)
            part = _dot(heads, ow_v[:, cols])
            for q in range(Q):
                psend[0, j, q, :, cols] = part[q * QR : (q + 1) * QR].astype(BF16)
                pown[j, q, :, cols] = part[OWN + q * QR : OWN + (q + 1) * QR]
        for q in range(Q):
            pair_send(0, j, q)

    def pair_send(rs, j, q):
        send(("dd", rs, j, q), psend.at[rs, j, q], precv.at[rs, j, q], sib)

    def pair_sum(rs, j, q):
        arrived(("dd", rs, j, q))
        return pown[j, q] + precv[rs, j, q].astype(F32)

    H2 = QR // 2

    def ring_1(rs, q):
        cs[rs, 0, q] = pair_sum(rs, 2, q).astype(BF16)
        for d in range(2):
            send(
                ("rx", rs, 1, d, q), cs.at[rs, 0, q, pl.ds(d * H2, H2)], r1.at[rs, d, q], x_to[d]
            )

    def ring_2(rs, q):
        for d in range(2):
            j = 1 if d == 0 else 3
            both = pair_sum(rs, j, q)
            arrived(("rx", rs, 1, d, q))
            more = r1[rs, d, q].astype(F32)
            if d == 0:
                both = jnp.concatenate([both[:H2] + more, both[H2:]], axis=0)
            else:
                both = jnp.concatenate([both[:H2], both[H2:] + more], axis=0)
            cs[rs, 1 + d, q] = both.astype(BF16)
            send(("rx", rs, 2, d, q), cs.at[rs, 1 + d, q], r2.at[rs, d, q], x_to[d])

    def ring_end(rs, q):
        total = pair_sum(rs, 0, q)
        for d in range(2):
            arrived(("rx", rs, 2, d, q))
            total = total + r2[rs, d, q].astype(F32)
        return total

    attend(2)
    attend(1)
    for q in range(Q):
        ring_1(0, q)
    dn_y_half(1)
    dn_y_half(7)
    dn_z(4)
    up_z(2)
    dn_y(3)
    dn_y(5)
    attend(3)
    attend(0)
    for q in range(Q):
        ring_2(0, q)

    loads["stream"].wait()

    def spread_rows(q):
        mid = (stream_v[pl.ds(q * QR, QR), :].astype(F32) + ring_end(0, q)).astype(BF16)
        mid_v[q] = mid
        midf = mid.astype(F32)
        nrm[1, 0, q] = (
            midf * lax.rsqrt(jnp.mean(midf * midf, axis=-1, keepdims=True) + EPS) * mg_ref[...]
        ).astype(BF16)
        for d in range(2):
            send(("ag", d, q), nrm.at[1, 0, q], nrm.at[1, 3 if d == 0 else 1, q], x_to[d])
        send(("ags", 0, q), nrm.at[1, 0, q], nrm.at[0, 0, q], sib)

    def spread_mid(q):
        for d in range(2):
            arrived(("ag", d, q))
            j = 3 if d == 0 else 1
            rows = pl.ds(d * H2, H2)
            send(("agh", d, q), nrm.at[1, j, q, rows], nrm.at[1, 2, q, rows], x_to[d])
            send(("ags", j, q), nrm.at[1, j, q], nrm.at[0, j, q], sib)

    def spread_end(q):
        for d in range(2):
            arrived(("agh", d, q))
        send(("ags", 2, q), nrm.at[1, 2, q], nrm.at[0, 2, q], sib)

    def spread_done(q):
        for j in range(4):
            arrived(("ags", j, q))

    def ff_up(q):
        def tile(n, carry):
            cols = pl.ds(pl.multiple_of(n * 256, 256), 256)
            pre = _dot(nrm[:, :, q].reshape(8 * QR, D), wu[:, :, cols].reshape(D, 256))
            pre = jnp.maximum(pre, 0.0)
            hid_v[:, cols] = (pre * pre).astype(BF16)
            return carry

        lax.fori_loop(0, HID // 256, tile, 0)

    def ff_down(q):
        def tile(n, carry):
            cols = pl.ds(pl.multiple_of(n * 256, 256), 256)
            part = _dot(
                hid_v[...], wd[pl.ds(n * 4, 4)].reshape(256, HID), (((1,), (1,)), ((), ()))
            ).reshape(2, 4, QR, 256)
            psend[1, :, q, :, cols] = part[0].astype(BF16)
            pown[:, q, :, cols] = part[1]
            return carry

        lax.fori_loop(0, D // 256, tile, 0)
        for j in (2, 1, 3, 0):
            pair_send(1, j, q)

    dn_z_done()
    dn_y(4)
    dn_y_half(2)
    dn_y_half(6)
    up_z(3)
    spread_rows(0)
    spread_rows(1)
    dn_y_half(3)
    dn_y_half(5)
    up_z(4)
    spread_mid(0)
    spread_mid(1)
    dn_y_half(4)
    spread_end(0)
    up_done()
    spread_done(0)
    ff_up(0)
    spread_end(1)
    dn_done()
    ff_down(0)
    ring_1(1, 0)
    spread_done(1)
    ff_up(1)
    ring_2(1, 0)
    ff_down(1)
    ring_1(1, 1)
    ring_2(1, 1)
    for q in range(Q):
        out_ref[pl.ds(q * QR, QR), :] = (mid_v[q].astype(F32) + ring_end(1, q)).astype(BF16)

    for name in copies:
        copies[name].wait_send()
    all_of(sx_send, "st1", ssem).wait()
    all_of(px_send, "st2", ssem).wait()


def local(
    stream,
    query_rows,
    key_rows,
    value_rows,
    gate_rows,
    log_decay,
    head_gain,
    out_weight,
    mix_gain,
    up_weight,
    down_weight,
):
    any_spec = pl.BlockSpec(memory_space=pl.ANY)
    vmem = pl.BlockSpec(memory_space=pltpu.VMEM)
    return pl.pallas_call(
        kernel,
        out_shape=jax.ShapeDtypeStruct((OWN, D), BF16),
        in_specs=[any_spec] * 6 + [vmem, any_spec, vmem, any_spec, any_spec],
        out_specs=vmem,
        scratch_shapes=[
            pltpu.VMEM((OWN, D), BF16),
            pltpu.VMEM((ROWS, KC), BF16),
            pltpu.VMEM((ROWS, KC), BF16),
            pltpu.VMEM((ROWS, DV), BF16),
            pltpu.VMEM((ROWS, DV), BF16),
            pltpu.VMEM((ROWS, KC), F32),
            pltpu.VMEM((DV, D), BF16),
            pltpu.VMEM((NSP, WR, HID), BF16),
            pltpu.VMEM((NSP, WR, HID), BF16),
            pltpu.VMEM((NB, DV, KC), F32),
            pltpu.VMEM((NB, 8, KC), F32),
            pltpu.VMEM((NSP, 16, KC), BF16),
            pltpu.VMEM((NSP, 16, KC), BF16),
            pltpu.VMEM((NSP, 8, KC), F32),
            pltpu.VMEM((NSP, 8, KC), F32),
            pltpu.VMEM((2, 4, Q, QR, D), BF16),
            pltpu.VMEM((2, 4, Q, QR, D), BF16),
            pltpu.VMEM((4, Q, QR, D), F32),
            pltpu.VMEM((2, 3, Q, QR, D), BF16),
            pltpu.VMEM((2, 2, Q, QR // 2, D), BF16),
            pltpu.VMEM((2, 2, Q, QR, D), BF16),
            pltpu.VMEM((2, 4, Q, QR, D), BF16),
            pltpu.VMEM((Q, QR, D), BF16),
            pltpu.VMEM((8 * QR, HID), BF16),
            pltpu.SemaphoreType.DMA((10,)),
            pltpu.SemaphoreType.DMA((N_IDS,)),
            pltpu.SemaphoreType.DMA((N_IDS,)),
        ],
        compiler_params=pltpu.CompilerParams(
            collective_id=0, has_side_effects=True, vmem_limit_bytes=60 * 1024 * 1024
        ),
        name="layer",
    )(
        stream,
        query_rows,
        key_rows,
        value_rows,
        gate_rows,
        log_decay,
        head_gain.reshape(1, DV),
        out_weight,
        mix_gain.reshape(1, D),
        up_weight,
        down_weight,
    )


def solution(mesh):
    torus = Mesh(mesh.devices.reshape(NZ, NY, NX, 2), SP_TP)
    in_specs = (
        P(SP_TP, None),
        P(SP, TP),
        P(SP, TP),
        P(SP, TP),
        P(SP, TP),
        P(SP, TP),
        P(),
        P(TP, None),
        P(),
        P(SP, TP),
        P(SP, TP),
    )
    out_specs = P(SP_TP, None)
    return jax.shard_map(local, mesh=torus, in_specs=in_specs, out_specs=out_specs, check_vma=False)
```

```python
import functools

import jax
import jax.numpy as jnp
from jax import lax
from jax.experimental import pallas as pl
from jax.experimental.pallas import tpu as pltpu
from jax.sharding import Mesh
from jax.sharding import PartitionSpec as P

KC = 128
DV = 256
BLOCK = 64
D = 2048
ROWS = 1024
OWN = 128
NB = ROWS // BLOCK
NZ, NY, NX = 8, 4, 4
NSP = NZ * NY
Q = 4
QR = OWN // Q
FR = OWN // 2
HID = 1024
WR = 64
AC = 768
EPS = 1e-06
SP = ("sp_0", "sp_1")
TP = ("tp_0", "tp_1")
SP_TP = ("sp_0", "sp_1", "tp_0", "tp_1")
MESH = pl.DeviceIdType.MESH
F32 = jnp.float32
BF16 = jnp.bfloat16

G = 4
CH1 = tuple((q * QR, QR, 0, D) for q in range(Q))
CH2 = tuple((f * FR, FR, g * (D // G), D // G) for f in range(2) for g in range(G))
CHUNKS = (CH1, CH2)
SLOT = {2: 0, 1: 1, 3: 2, 0: 3}

RECV, SEND = {}, {}


def _recv_id(*name):
    RECV.setdefault(name, len(RECV))
    SEND.setdefault(name[0], len(SEND))


for _n in ("ay", "ayh", "st1", "st2", "st3"):
    _recv_id(_n)
for _i in (1, 2, 3, 4):
    _recv_id("bz", _i)
    for _h in range(2 if _i < 4 else 1):
        _recv_id("az", _i, _h)
for _k in range(8):
    _recv_id("by", _k)
    _recv_id("byh", _k)
for _n in ((2, 0), (2, 1), 1, 3, 0):
    _recv_id("dd0", _n)
for _n in range(len(CH2)):
    _recv_id("dd1", 0, _n)
    _recv_id("dd1", 1, _n)
for _rs in range(2):
    for _n in range(len(CHUNKS[_rs])):
        for _s in (1, 2):
            _recv_id(("rx", _rs, _s), _n)
for _q in range(Q):
    _recv_id("ag", _q)
    _recv_id("agh", _q)
for _f in range(2):
    _recv_id("ags", _f)


def _dot(a, b, dims=(((1,), (0,)), ((), ()))):
    return lax.dot_general(a, b, dims, preferred_element_type=F32)


def _split(x):
    hi = x.astype(BF16)
    return hi, (x - hi.astype(F32)).astype(BF16)


def kernel(
    stream_h,
    q_h,
    k_h,
    v_h,
    g_h,
    ld_h,
    hg_h,
    ow_h,
    mg_h,
    up_h,
    dn_h,
    out_ref,
    hg_ref,
    mg_ref,
    stream_v,
    q_v,
    k_v,
    v_v,
    g_v,
    ld_v,
    ow_v,
    w,
    wt,
    sloc,
    cl,
    sx_send,
    sx_recv,
    zx_send,
    zx_recv,
    px_send,
    px_recv,
    psend,
    precv,
    pown,
    cs,
    r1,
    r2,
    nrm,
    mid_v,
    hid_v,
    lsem,
    ssem,
    rsem,
):
    z, y = lax.axis_index("sp_0"), lax.axis_index("sp_1")
    x, c = lax.axis_index("tp_0"), lax.axis_index("tp_1")
    sp = z * NY + y
    yl, yr = lax.rem(y + NY - 1, NY), lax.rem(y + 1, NY)
    zl, zr = lax.rem(z + NZ - 1, NZ), lax.rem(z + 1, NZ)
    xl, xr = lax.rem(x + NX - 1, NX), lax.rem(x + 1, NX)
    y_to, y_from = ({"sp_1": yr}, {"sp_1": yl}), (yl, yr)
    z_to = ({"sp_0": zr}, {"sp_0": zl})
    x_to = ({"tp_0": xr}, {"tp_0": xl})
    sib = {"tp_1": 1 - c}

    barrier = pltpu.get_barrier_semaphore()

    def signal_to(other):
        pl.semaphore_signal(barrier, inc=1, device_id=other, device_id_type=MESH)

    def greet_y(d, carry):
        signal_to({"sp_1": lax.rem(y + d, NY)})
        return carry

    def greet_z(d, carry):
        signal_to({"sp_0": lax.rem(z + d, NZ)})
        return carry

    lax.fori_loop(1, NY, greet_y, 0)
    lax.fori_loop(1, NZ, greet_z, 0)
    for other in (x_to[0], x_to[1], sib):
        signal_to(other)

    loads = {}

    def load(name, src, dst, i):
        loads[name] = pltpu.make_async_copy(src, dst, lsem.at[i])
        loads[name].start()

    load("ld", ld_h, ld_v, 0)
    load("k", k_h, k_v, 1)
    load("v", v_h, v_v, 2)
    load("up", up_h, w.at[sp, :, pl.ds(0, HID)], 3)
    load("dn", dn_h, w.at[sp, :, pl.ds(HID, HID)], 4)
    load("q", q_h, q_v, 5)
    load("g", g_h, g_v, 6)
    load("ow", ow_h, ow_v, 7)
    load("stream", stream_h, stream_v, 8)
    load("hg", hg_h, hg_ref, 9)
    load("mg", mg_h, mg_ref, 10)

    def send(name, src, dst, to):
        pltpu.make_async_remote_copy(
            src_ref=src,
            dst_ref=dst,
            send_sem=ssem.at[SEND[name[0]]],
            recv_sem=rsem.at[RECV[name]],
            device_id=to,
            device_id_type=MESH,
        ).start()

    waited = set()

    def arrived(name, size):
        if name not in waited:
            waited.add(name)
            pltpu.make_async_copy(size, size, rsem.at[RECV[name]]).wait()

    def sent(family, size):
        pltpu.make_async_copy(size, size, ssem.at[SEND[family]]).wait()

    HALF = (pl.ds(0, WR // 2), pl.ds(WR // 2, WR // 2))
    COLS_A, COLS_B = pl.ds(0, AC), pl.ds(AC, 2 * HID - AC)

    def zat(off):
        return lax.rem(z + off + NZ, NZ)

    def some_a(n):
        return w.at[pl.ds(0, n), :, COLS_A]

    def some_b(n):
        return w.at[pl.ds(0, n), :, COLS_B]

    def up_y():
        for d in range(2):
            part = w.at[sp, :, COLS_A]
            send(("ay",), part, part, y_to[d])

    def up_y_half():
        arrived(("ay",), some_a(2))
        for d in range(2):
            part = w.at[z * NY + y_from[d], HALF[d], COLS_A]
            send(("ayh",), part, part, y_to[d])

    def up_z(i, step):
        if i == 1:
            arrived(("ayh",), some_a(1))
        else:
            arrived(("az", i - 1, step), some_a(4))
        if i < 4 or step == 0:
            for d in range(2):
                zz = zat(-(i - 1) if d == 0 else i - 1)
                part = w.at[pl.ds(zz * NY, NY), HALF[step if d == 0 else 1 - step], COLS_A]
                send(("az", i, step), part, part, z_to[d])

    def up_done():
        arrived(("az", 4, 0), some_a(4))

    def dn_z(i):
        if i > 1:
            arrived(("bz", i - 1), some_b(2))
        for d in range(2):
            blk = zat(-(i - 1) if d == 0 else i - 1) * NY + y
            part = w.at[blk, :, COLS_B] if i < 4 else w.at[blk, HALF[d], COLS_B]
            send(("bz", i), part, part, z_to[d])

    def dn_y(k):
        if k in (1, 7):
            arrived(("bz", 1), some_b(2))
        if k == 4:
            arrived(("bz", 4), some_b(1))
        part = w.at[zat(k) * NY + y, :, COLS_B]
        for d in range(2):
            send(("by", k), part, part, y_to[d])

    def dn_y_half(k):
        arrived(("by", k), some_b(2))
        for d in range(2):
            part = w.at[zat(k) * NY + y_from[d], HALF[d], COLS_B]
            send(("byh", k), part, part, y_to[d])

    def dn_turn(k):
        arrived(("byh", k), some_b(1))
        zz = zat(k)
        slab = w[pl.ds(zz * NY, NY), :, pl.ds(HID, HID)].reshape(NY * WR, HID)
        wt[:, pl.ds(pl.multiple_of(zz * NY * WR, NY * WR), NY * WR)] = slab.T

    loads["ld"].wait()
    loads["k"].wait()
    loads["v"].wait()
    r_i = lax.broadcasted_iota(jnp.int32, (256, 256), 0)
    c_i = lax.broadcasted_iota(jnp.int32, (256, 256), 1)
    tri = jnp.where((c_i > r_i) & (c_i // BLOCK == r_i // BLOCK), 1.0, 0.0).astype(BF16)

    def group(gi, carry):
        state, total = carry
        rows = pl.ds(pl.multiple_of(gi * 256, 256), 256)
        ld = ld_v[rows, :]
        hi, lo = _split(ld)
        lo2 = (ld - hi.astype(F32) - lo.astype(F32)).astype(BF16)
        suf = _dot(tri, hi) + _dot(tri, lo) + _dot(tri, lo2)
        dk = k_v[rows, :].astype(F32) * jnp.exp(suf)
        dk_hi, dk_lo = _split(dk)
        vals = v_v[rows, :]
        for b in range(4):
            s = slice(b * BLOCK, (b + 1) * BLOCK)
            vv = jnp.concatenate([vals[s], vals[s]], axis=0)
            dd = jnp.concatenate([dk_hi[s], dk_lo[s]], axis=0)
            upd = _dot(vv, dd, (((0,), (0,)), ((), ())))
            last = suf[b * BLOCK : b * BLOCK + 1] + ld[b * BLOCK : b * BLOCK + 1]
            state = jnp.exp(last) * state + upd
            total = total + last
            sloc[gi * 4 + b] = state
            cl[gi * 4 + b] = jnp.broadcast_to(total, (8, KC))
        return state, total

    state, total = lax.fori_loop(
        0, NB // 4, group, (jnp.zeros((DV, KC), F32), jnp.zeros((1, KC), F32))
    )

    QV = DV // NY

    def with_log(block, log):
        hi, lo = _split(log)
        lo2 = (log - hi.astype(F32) - lo.astype(F32)).astype(BF16)
        sub = lax.broadcasted_iota(jnp.int32, (16, KC), 0)
        logs = jnp.where(
            sub == 0,
            hi.astype(F32),
            jnp.where(sub == 1, lo.astype(F32), jnp.where(sub == 2, lo2.astype(F32), 0.0)),
        )
        return jnp.concatenate([block, logs], axis=0).astype(BF16)

    def block_log(tile):
        t = tile.astype(F32)
        return t[:QV], t[QV : QV + 1] + t[QV + 1 : QV + 2] + t[QV + 2 : QV + 3]

    def first(ref, count):
        return ref.at[pl.ds(0, count)]

    def scatter(name, count, src_of, dst, to):
        def one(d, carry):
            pltpu.make_async_remote_copy(
                src_ref=src_of(d),
                dst_ref=dst,
                send_sem=ssem.at[SEND[name]],
                recv_sem=rsem.at[RECV[(name,)]],
                device_id=to(d),
                device_id_type=MESH,
            ).start()
            return carry

        lax.fori_loop(1, count, one, 0)

    def y_at(d):
        return lax.rem(y + d, NY)

    for p in range(NY):
        sx_send[p] = with_log(state[p * QV : (p + 1) * QV], total)

    pl.semaphore_wait(barrier, NY - 1 + NZ - 1 + 3)
    scatter("st1", NY, lambda d: sx_send.at[y_at(d)], sx_recv.at[y], lambda d: {"sp_1": y_at(d)})
    sx_recv[y] = sx_send[y]
    loads["up"].wait()
    loads["dn"].wait()
    up_y()
    dn_y(0)
    dn_z(1)
    arrived(("st1",), first(sx_recv, NY - 1))

    group_state, group_log = block_log(sx_recv[0])
    for p in range(1, NY):
        more, log = block_log(sx_recv[p])
        group_state = jnp.exp(log) * group_state + more
        group_log = group_log + log
    zx_send[...] = with_log(group_state, group_log)
    scatter(
        "st2", NZ, lambda d: zx_send, zx_recv.at[z], lambda d: {"sp_0": lax.rem(z + d, NZ)}
    )
    zx_recv[z] = zx_send[...]
    up_y_half()
    dn_y(1)
    arrived(("st2",), first(zx_recv, NZ - 1))

    run = jnp.zeros((QV, KC), F32)
    for e in range(NZ):
        more, log = block_log(zx_recv[e])
        run = jnp.where(e < z, jnp.exp(log) * run + more, run)
    for p in range(NY):
        px_send[p] = run.astype(BF16)
        more, log = block_log(sx_recv[p])
        run = jnp.exp(log) * run + more
    scatter("st3", NY, lambda d: px_send.at[y_at(d)], px_recv.at[y], lambda d: {"sp_1": y_at(d)})
    px_recv[y] = px_send[y]

    dn_z(2)
    dn_y(7)
    dn_y_half(0)
    up_z(1, 0)
    loads["q"].wait()
    loads["g"].wait()
    loads["ow"].wait()
    loads["hg"].wait()
    arrived(("st3",), first(px_recv, NY - 1))

    def attend(j):
        s_in = px_recv[...].astype(F32).reshape(DV, KC)
        base = lax.rem(x + j, NX) * 4
        gain = hg_ref[...]
        outs = []
        for half in range(2):
            first = base + (1 - c if half == 0 else c) * 2
            for b in range(2):
                n = first + b
                rows = pl.ds(pl.multiple_of(n * BLOCK, BLOCK), BLOCK)
                full = sloc[n] + jnp.exp(cl[n][0:1]) * s_in
                f_hi, f_lo = _split(full)
                qq = q_v[rows, :]
                read = _dot(
                    jnp.concatenate([qq, qq], axis=1),
                    jnp.concatenate([f_hi, f_lo], axis=1),
                    (((1,), (1,)), ((), ())),
                ) * (KC**-0.5)
                scaled = read * lax.rsqrt(jnp.mean(read * read, axis=-1, keepdims=True) + EPS)
                gate = g_v[rows, :].astype(F32)
                outs.append((scaled * gain * (gate / (1.0 + jnp.exp(-gate)))).astype(BF16))
        heads = jnp.concatenate(outs, axis=0)
        for n in range(4):
            cols = slice(n * 512, (n + 1) * 512)
            part = _dot(heads, ow_v[:, cols])
            psend[0, SLOT[j], :, cols] = part[:OWN].astype(BF16)
            pown[SLOT[j], :, cols] = part[OWN:]
        for name, rows in pair_parts(j):
            send(("dd0", name), psend.at[0, SLOT[j], rows], precv.at[0, SLOT[j], rows], sib)

    def views(rs, n):
        r0, nr, c0, nc = CHUNKS[rs][n]
        return pl.ds(r0, nr), pl.ds(c0, nc), pl.ds(r0 // 2, nr // 2), nr // 2, r0

    def pair_parts(j):
        if j == 2:
            return (((2, 0), pl.ds(0, QR)), ((2, 1), pl.ds(QR, OWN - QR)))
        return ((j, pl.ds(0, OWN)),)

    def pair_sum(rs, j, n):
        rows, cols, _, _, _ = views(rs, n)
        if rs == 0:
            name, part = pair_parts(j)[1 if j == 2 and n > 0 else 0]
            arrived(("dd0", name), precv.at[0, SLOT[j], part])
        elif j == 2:
            arrived(("dd1", 0, n), precv.at[1, 0, rows, cols])
        else:
            arrived(("dd1", 1, n), precv.at[1, pl.ds(1, 3), rows, cols])
        return pown[SLOT[j], rows, cols] + precv[rs, SLOT[j], rows, cols].astype(F32)

    def ring_1(rs, n):
        rows, cols, half, h2, r0 = views(rs, n)
        cs[rs, 0, rows, cols] = pair_sum(rs, 2, n).astype(BF16)
        for d in range(2):
            send(
                (("rx", rs, 1), n),
                cs.at[rs, 0, pl.ds(r0 + d * h2, h2), cols],
                r1.at[rs, d, half, cols],
                x_to[d],
            )

    def ring_2(rs, n):
        rows, cols, half, h2, _ = views(rs, n)
        both = [pair_sum(rs, 1, n), pair_sum(rs, 3, n)]
        arrived((("rx", rs, 1), n), r1.at[rs, :, half, cols])
        for d in range(2):
            more = r1[rs, d, half, cols].astype(F32)
            if d == 0:
                total = jnp.concatenate([both[d][:h2] + more, both[d][h2:]], axis=0)
            else:
                total = jnp.concatenate([both[d][:h2], both[d][h2:] + more], axis=0)
            cs[rs, 1 + d, rows, cols] = total.astype(BF16)
            send((("rx", rs, 2), n), cs.at[rs, 1 + d, rows, cols], r2.at[rs, d, rows, cols], x_to[d])

    def ring_end(rs, n):
        rows, cols, _, _, _ = views(rs, n)
        total = pair_sum(rs, 0, n)
        arrived((("rx", rs, 2), n), r2.at[rs, :, rows, cols])
        return total + r2[rs, 0, rows, cols].astype(F32) + r2[rs, 1, rows, cols].astype(F32)

    def rows_of(q):
        return pl.ds(q * QR, QR)

    def norm_rows(q):
        rows = rows_of(q)
        mid = (stream_v[rows, :].astype(F32) + ring_end(0, q)).astype(BF16)
        mid_v[rows, :] = mid
        midf = mid.astype(F32)
        nrm[1, 0, rows, :] = (
            midf * lax.rsqrt(jnp.mean(midf * midf, axis=-1, keepdims=True) + EPS) * mg_ref[...]
        ).astype(BF16)

    def spread_rows(q):
        rows = rows_of(q)
        for d in range(2):
            send(("ag", q), nrm.at[1, 0, rows], nrm.at[1, 3 if d == 0 else 1, rows], x_to[d])
        send(("ags", q // 2), nrm.at[1, 0, rows], nrm.at[0, 0, rows], sib)

    def spread_mid(q):
        rows = rows_of(q)
        arrived(("ag", q), nrm.at[1, pl.ds(0, 2), rows])
        for d in range(2):
            j = 3 if d == 0 else 1
            part = pl.ds(q * QR + d * (QR // 2), QR // 2)
            send(("agh", q), nrm.at[1, j, part], nrm.at[1, 2, part], x_to[d])
            send(("ags", q // 2), nrm.at[1, j, rows], nrm.at[0, j, rows], sib)

    def spread_end(q):
        rows = rows_of(q)
        arrived(("agh", q), nrm.at[1, 2, rows])
        send(("ags", q // 2), nrm.at[1, 2, rows], nrm.at[0, 2, rows], sib)

    def spread_done(f):
        arrived(("ags", f), nrm.at[0, :, pl.ds(f * FR, FR)])

    def ff_up(f, n):
        x_in = nrm[:, :, pl.ds(f * FR, FR)].reshape(8 * FR, D)
        for c0 in (n * 512, n * 512 + 256):
            pre = _dot(x_in, w[:, :, c0 : c0 + 256].reshape(D, 256))
            pre = jnp.maximum(pre, 0.0)
            hid_v[:, c0 : c0 + 256] = (pre * pre).astype(BF16)

    def ff_down(f, g):
        rows = slice(f * FR, (f + 1) * FR)
        for c0 in range(g * (D // G), (g + 1) * (D // G), 256):
            part = _dot(hid_v[...], wt[:, c0 : c0 + 256]).reshape(2, 4, FR, 256)
            for j in range(4):
                psend[1, SLOT[j], rows, c0 : c0 + 256] = part[0, j].astype(BF16)
                pown[SLOT[j], rows, c0 : c0 + 256] = part[1, j]
        n = G * f + g
        rows, cols, _, _, _ = views(1, n)
        for i, slots in enumerate((pl.ds(0, 1), pl.ds(1, 3))):
            send(("dd1", i, n), psend.at[1, slots, rows, cols], precv.at[1, slots, rows, cols], sib)

    def out_rows(n):
        rows, cols, _, _, _ = views(1, n)
        out_ref[rows, cols] = (mid_v[rows, cols].astype(F32) + ring_end(1, n)).astype(BF16)

    attend(2)
    attend(1)
    dn_z(3)
    dn_y(2)
    dn_y(6)
    up_z(1, 1)
    ring_1(0, 0)
    ring_1(0, 1)
    ring_1(0, 2)
    ring_1(0, 3)
    attend(3)
    attend(0)
    dn_y_half(1)
    dn_y_half(7)
    up_z(2, 0)
    ring_2(0, 0)
    ring_2(0, 1)
    ring_2(0, 2)
    dn_z(4)
    dn_y(3)
    dn_y(5)
    ring_2(0, 3)
    dn_y_half(2)
    dn_y_half(6)
    up_z(2, 1)
    loads["stream"].wait()
    loads["mg"].wait()
    norm_rows(0)
    spread_rows(0)
    dn_turn(0)
    norm_rows(1)
    spread_rows(1)
    up_z(3, 0)
    dn_y(4)
    norm_rows(2)
    dn_turn(1)
    dn_turn(7)
    up_z(3, 1)
    norm_rows(3)
    spread_mid(0)
    up_z(4, 0)
    dn_y_half(3)
    dn_y_half(5)
    spread_mid(1)
    spread_rows(2)
    spread_rows(3)
    dn_turn(2)
    dn_turn(6)
    spread_end(0)
    dn_y_half(4)
    spread_end(1)
    up_z(4, 1)
    dn_turn(3)
    dn_turn(5)
    up_done()
    spread_done(0)
    dn_turn(4)
    ff_up(0, 0)
    spread_mid(2)
    ff_up(0, 1)
    spread_mid(3)
    ff_down(0, 0)
    ff_down(0, 1)
    ff_down(0, 2)
    ring_1(1, 0)
    ff_down(0, 3)
    ring_1(1, 1)
    spread_end(2)
    spread_end(3)
    ring_1(1, 2)
    ring_1(1, 3)
    spread_done(1)
    ff_up(1, 0)
    ring_2(1, 0)
    ring_2(1, 1)
    ff_up(1, 1)
    ring_2(1, 2)
    ff_down(1, 0)
    ring_2(1, 3)
    ff_down(1, 1)
    ring_1(1, 4)
    ff_down(1, 2)
    ring_1(1, 5)
    ff_down(1, 3)
    ring_1(1, 6)
    out_rows(0)
    ring_1(1, 7)
    ring_2(1, 4)
    ring_2(1, 5)
    out_rows(1)
    out_rows(2)
    ring_2(1, 6)
    out_rows(3)
    ring_2(1, 7)
    out_rows(4)
    out_rows(5)
    out_rows(6)
    out_rows(7)

    for family, size in (
        ("ay", some_a(2)),
        ("ayh", some_a(1)),
        ("az", some_a(28)),
        ("bz", some_b(7)),
        ("by", some_b(16)),
        ("byh", some_b(8)),
        ("st1", first(sx_send, NY - 1)),
        ("st2", first(zx_recv, NZ - 1)),
        ("st3", first(px_send, NY - 1)),
        ("dd0", psend.at[0]),
        ("dd1", psend.at[1]),
        (("rx", 0, 1), cs.at[0, 0]),
        (("rx", 0, 2), cs.at[0, pl.ds(1, 2)]),
        (("rx", 1, 1), cs.at[1, 0]),
        (("rx", 1, 2), cs.at[1, pl.ds(1, 2)]),
        ("ag", nrm.at[1, pl.ds(0, 2)]),
        ("agh", nrm.at[1, 0]),
        ("ags", nrm.at[0]),
    ):
        sent(family, size)


def local(
    stream,
    query_rows,
    key_rows,
    value_rows,
    gate_rows,
    log_decay,
    head_gain,
    out_weight,
    mix_gain,
    up_weight,
    down_weight,
):
    any_spec = pl.BlockSpec(memory_space=pl.ANY)
    vmem = pl.BlockSpec(memory_space=pltpu.VMEM)
    return pl.pallas_call(
        kernel,
        out_shape=pltpu.VMEM((OWN, D), BF16),
        in_specs=[any_spec] * 11,
        out_specs=vmem,
        scratch_shapes=[
            pltpu.VMEM((1, DV), F32),
            pltpu.VMEM((1, D), F32),
            pltpu.VMEM((OWN, D), BF16),
            pltpu.VMEM((ROWS, KC), BF16),
            pltpu.VMEM((ROWS, KC), BF16),
            pltpu.VMEM((ROWS, DV), BF16),
            pltpu.VMEM((ROWS, DV), BF16),
            pltpu.VMEM((ROWS, KC), F32),
            pltpu.VMEM((DV, D), BF16),
            pltpu.VMEM((NSP, WR, 2 * HID), BF16),
            pltpu.VMEM((HID, D), BF16),
            pltpu.VMEM((NB, DV, KC), F32),
            pltpu.VMEM((NB, 8, KC), F32),
            pltpu.VMEM((NY, DV // NY + 16, KC), BF16),
            pltpu.VMEM((NY, DV // NY + 16, KC), BF16),
            pltpu.VMEM((DV // NY + 16, KC), BF16),
            pltpu.VMEM((NZ, DV // NY + 16, KC), BF16),
            pltpu.VMEM((NY, DV // NY, KC), BF16),
            pltpu.VMEM((NY, DV // NY, KC), BF16),
            pltpu.VMEM((2, 4, OWN, D), BF16),
            pltpu.VMEM((2, 4, OWN, D), BF16),
            pltpu.VMEM((4, OWN, D), F32),
            pltpu.VMEM((2, 3, OWN, D), BF16),
            pltpu.VMEM((2, 2, OWN // 2, D), BF16),
            pltpu.VMEM((2, 2, OWN, D), BF16),
            pltpu.VMEM((2, 4, OWN, D), BF16),
            pltpu.VMEM((OWN, D), BF16),
            pltpu.VMEM((8 * FR, HID), BF16),
            pltpu.SemaphoreType.DMA((11,)),
            pltpu.SemaphoreType.DMA((len(SEND),)),
            pltpu.SemaphoreType.DMA((len(RECV),)),
        ],
        compiler_params=pltpu.CompilerParams(
            collective_id=0, has_side_effects=True, vmem_limit_bytes=60 * 1024 * 1024
        ),
        name="layer",
    )(
        stream,
        query_rows,
        key_rows,
        value_rows,
        gate_rows,
        log_decay,
        head_gain.reshape(1, DV),
        out_weight,
        mix_gain.reshape(1, D),
        up_weight,
        down_weight,
    )


def solution(mesh):
    torus = Mesh(mesh.devices.reshape(NZ, NY, NX, 2), SP_TP)
    in_specs = (
        P(SP_TP, None),
        P(SP, TP),
        P(SP, TP),
        P(SP, TP),
        P(SP, TP),
        P(SP, TP),
        P(),
        P(TP, None),
        P(),
        P(SP, TP),
        P(SP, TP),
    )
    out_specs = P(SP_TP, None)
    return jax.shard_map(local, mesh=torus, in_specs=in_specs, out_specs=out_specs, check_vma=False)
```

```python
import functools

import jax
import jax.numpy as jnp
from jax import lax
from jax.experimental import pallas as pl
from jax.experimental.pallas import tpu as pltpu
from jax.sharding import Mesh
from jax.sharding import PartitionSpec as P

KC = 128
DV = 256
BLOCK = 64
D = 2048
ROWS = 1024
OWN = 128
NB = ROWS // BLOCK
NZ, NY, NX = 8, 4, 4
NSP = NZ * NY
Q = 4
QR = OWN // Q
HID = 1024
WR = 64
AC = 768
EPS = 1e-06
SP = ("sp_0", "sp_1")
TP = ("tp_0", "tp_1")
SP_TP = ("sp_0", "sp_1", "tp_0", "tp_1")
MESH = pl.DeviceIdType.MESH
F32 = jnp.float32
BF16 = jnp.bfloat16

G = 2
CH1 = tuple((q * QR, QR, 0, D) for q in range(Q))
CH2 = tuple((q * QR, QR, g * (D // G), D // G) for q in range(Q) for g in range(G))
CHUNKS = (CH1, CH2)
SLOT = {2: 0, 1: 1, 3: 2, 0: 3}

RECV, SEND = {}, {}


def _recv_id(*name):
    RECV.setdefault(name, len(RECV))
    SEND.setdefault(name[0], len(SEND))


for _n in ("ay", "ayh", "st1", "st2", "st3"):
    _recv_id(_n)
for _i in (1, 2, 3, 4):
    _recv_id("bz", _i)
    for _h in range(2 if _i < 4 else 1):
        _recv_id("az", _i, _h)
for _k in range(8):
    _recv_id("by", _k)
    _recv_id("byh", _k)
for _n in ((2, 0), (2, 1), 1, 3, 0):
    _recv_id("dd0", _n)
for _n in range(len(CH2)):
    _recv_id("dd1", 0, _n)
    _recv_id("dd1", 1, _n)
for _rs in range(2):
    for _n in range(len(CHUNKS[_rs])):
        for _s in (1, 2):
            _recv_id(("rx", _rs, _s), _n)
for _q in range(Q):
    _recv_id("ag", _q)
    _recv_id("agh", _q)
    _recv_id("ags", _q)


def _dot(a, b, dims=(((1,), (0,)), ((), ()))):
    return lax.dot_general(a, b, dims, preferred_element_type=F32)


def _split(x):
    hi = x.astype(BF16)
    return hi, (x - hi.astype(F32)).astype(BF16)


def kernel(
    stream_h,
    q_h,
    k_h,
    v_h,
    g_h,
    ld_h,
    hg_h,
    ow_h,
    mg_h,
    up_h,
    dn_h,
    out_ref,
    hg_ref,
    mg_ref,
    stream_v,
    q_v,
    k_v,
    v_v,
    g_v,
    gate_v,
    ld_v,
    ow_v,
    w,
    wt,
    sloc,
    cl,
    sx_send,
    sx_recv,
    zx_send,
    zx_recv,
    px_send,
    px_recv,
    psend,
    precv,
    pown,
    cs,
    r1,
    r2,
    nrm,
    mid_v,
    hid_v,
    lsem,
    ssem,
    rsem,
):
    z, y = lax.axis_index("sp_0"), lax.axis_index("sp_1")
    x, c = lax.axis_index("tp_0"), lax.axis_index("tp_1")
    sp = z * NY + y
    yl, yr = lax.rem(y + NY - 1, NY), lax.rem(y + 1, NY)
    zl, zr = lax.rem(z + NZ - 1, NZ), lax.rem(z + 1, NZ)
    xl, xr = lax.rem(x + NX - 1, NX), lax.rem(x + 1, NX)
    y_to, y_from = ({"sp_1": yr}, {"sp_1": yl}), (yl, yr)
    z_to = ({"sp_0": zr}, {"sp_0": zl})
    x_to = ({"tp_0": xr}, {"tp_0": xl})
    sib = {"tp_1": 1 - c}

    barrier = pltpu.get_barrier_semaphore()

    def signal_to(other):
        pl.semaphore_signal(barrier, inc=1, device_id=other, device_id_type=MESH)

    def greet_y(d, carry):
        signal_to({"sp_1": lax.rem(y + d, NY)})
        return carry

    def greet_z(d, carry):
        signal_to({"sp_0": lax.rem(z + d, NZ)})
        return carry

    lax.fori_loop(1, NY, greet_y, 0)
    lax.fori_loop(1, NZ, greet_z, 0)
    for other in (x_to[0], x_to[1], sib):
        signal_to(other)

    loads = {}

    def load(name, src, dst, i):
        loads[name] = pltpu.make_async_copy(src, dst, lsem.at[i])
        loads[name].start()

    load("ld", ld_h, ld_v, 0)
    load("k", k_h, k_v, 1)
    load("v", v_h, v_v, 2)

    def send(name, src, dst, to):
        pltpu.make_async_remote_copy(
            src_ref=src,
            dst_ref=dst,
            send_sem=ssem.at[SEND[name[0]]],
            recv_sem=rsem.at[RECV[name]],
            device_id=to,
            device_id_type=MESH,
        ).start()

    waited = set()

    def arrived(name, size):
        if name not in waited:
            waited.add(name)
            pltpu.make_async_copy(size, size, rsem.at[RECV[name]]).wait()

    def sent(family, size):
        pltpu.make_async_copy(size, size, ssem.at[SEND[family]]).wait()

    HALF = (pl.ds(0, WR // 2), pl.ds(WR // 2, WR // 2))
    COLS_A, COLS_B = pl.ds(0, AC), pl.ds(AC, 2 * HID - AC)

    def zat(off):
        return lax.rem(z + off + NZ, NZ)

    def some_a(n):
        return w.at[pl.ds(0, n), :, COLS_A]

    def some_b(n):
        return w.at[pl.ds(0, n), :, COLS_B]

    def up_y():
        for d in range(2):
            part = w.at[sp, :, COLS_A]
            send(("ay",), part, part, y_to[d])

    def up_y_half():
        arrived(("ay",), some_a(2))
        for d in range(2):
            part = w.at[z * NY + y_from[d], HALF[d], COLS_A]
            send(("ayh",), part, part, y_to[d])

    def up_z(i, step):
        if i == 1:
            arrived(("ayh",), some_a(1))
        else:
            arrived(("az", i - 1, step), some_a(4))
        if i < 4 or step == 0:
            for d in range(2):
                zz = zat(-(i - 1) if d == 0 else i - 1)
                part = w.at[pl.ds(zz * NY, NY), HALF[step if d == 0 else 1 - step], COLS_A]
                send(("az", i, step), part, part, z_to[d])

    def up_done():
        arrived(("az", 4, 0), some_a(4))

    def dn_z(i):
        if i > 1:
            arrived(("bz", i - 1), some_b(2))
        for d in range(2):
            blk = zat(-(i - 1) if d == 0 else i - 1) * NY + y
            part = w.at[blk, :, COLS_B] if i < 4 else w.at[blk, HALF[d], COLS_B]
            send(("bz", i), part, part, z_to[d])

    def dn_y(k):
        if k in (1, 7):
            arrived(("bz", 1), some_b(2))
        if k == 4:
            arrived(("bz", 4), some_b(1))
        part = w.at[zat(k) * NY + y, :, COLS_B]
        for d in range(2):
            send(("by", k), part, part, y_to[d])

    def dn_y_half(k):
        arrived(("by", k), some_b(2))
        for d in range(2):
            part = w.at[zat(k) * NY + y_from[d], HALF[d], COLS_B]
            send(("byh", k), part, part, y_to[d])

    def dn_turn(k):
        arrived(("byh", k), some_b(1))
        zz = zat(k)
        slab = w[pl.ds(zz * NY, NY), :, pl.ds(HID, HID)].reshape(NY * WR, HID)
        wt[:, pl.ds(pl.multiple_of(zz * NY * WR, NY * WR), NY * WR)] = slab.T

    loads["ld"].wait()
    loads["k"].wait()
    loads["v"].wait()
    load("up", up_h, w.at[sp, :, pl.ds(0, HID)], 3)
    load("dn", dn_h, w.at[sp, :, pl.ds(HID, HID)], 4)
    load("q", q_h, q_v, 5)
    load("g", g_h, g_v, 6)
    load("ow", ow_h, ow_v, 7)
    load("stream", stream_h, stream_v, 8)
    load("hg", hg_h, hg_ref, 9)
    load("mg", mg_h, mg_ref, 10)
    r_i = lax.broadcasted_iota(jnp.int32, (256, 256), 0)
    c_i = lax.broadcasted_iota(jnp.int32, (256, 256), 1)
    tri = jnp.where((c_i > r_i) & (c_i // BLOCK == r_i // BLOCK), 1.0, 0.0).astype(BF16)

    def group(gi, state, total):
        rows = slice(gi * 256, (gi + 1) * 256)
        ld = ld_v[rows, :]
        hi, lo = _split(ld)
        lo2 = (ld - hi.astype(F32) - lo.astype(F32)).astype(BF16)
        suf = _dot(tri, hi) + _dot(tri, lo) + _dot(tri, lo2)
        dk = k_v[rows, :].astype(F32) * jnp.exp(suf)
        dk_hi, dk_lo = _split(dk)
        vals = v_v[rows, :]
        for b in range(4):
            s = slice(b * BLOCK, (b + 1) * BLOCK)
            vv = jnp.concatenate([vals[s], vals[s]], axis=0)
            dd = jnp.concatenate([dk_hi[s], dk_lo[s]], axis=0)
            upd = _dot(vv, dd, (((0,), (0,)), ((), ())))
            last = suf[b * BLOCK : b * BLOCK + 1] + ld[b * BLOCK : b * BLOCK + 1]
            state = jnp.exp(last) * state + upd
            total = total + last
            sloc[gi * 4 + b] = state
            cl[gi * 4 + b] = jnp.broadcast_to(total, (8, KC))
        return state, total

    state, total = jnp.zeros((DV, KC), F32), jnp.zeros((1, KC), F32)
    for gi in range(NB // 4):
        state, total = group(gi, state, total)

    QV = DV // NY

    def with_log(block, log):
        hi, lo = _split(log)
        lo2 = (log - hi.astype(F32) - lo.astype(F32)).astype(BF16)
        sub = lax.broadcasted_iota(jnp.int32, (16, KC), 0)
        logs = jnp.where(
            sub == 0,
            hi.astype(F32),
            jnp.where(sub == 1, lo.astype(F32), jnp.where(sub == 2, lo2.astype(F32), 0.0)),
        )
        return jnp.concatenate([block, logs], axis=0).astype(BF16)

    def block_log(tile):
        t = tile.astype(F32)
        return t[:QV], t[QV : QV + 1] + t[QV + 1 : QV + 2] + t[QV + 2 : QV + 3]

    def first(ref, count):
        return ref.at[pl.ds(0, count)]

    def scatter(name, count, src_of, dst, to):
        def one(d, carry):
            pltpu.make_async_remote_copy(
                src_ref=src_of(d),
                dst_ref=dst,
                send_sem=ssem.at[SEND[name]],
                recv_sem=rsem.at[RECV[(name,)]],
                device_id=to(d),
                device_id_type=MESH,
            ).start()
            return carry

        lax.fori_loop(1, count, one, 0)

    def y_at(d):
        return lax.rem(y + d, NY)

    for p in range(NY):
        sx_send[p] = with_log(state[p * QV : (p + 1) * QV], total)

    pl.semaphore_wait(barrier, NY - 1 + NZ - 1 + 3)
    scatter("st1", NY, lambda d: sx_send.at[y_at(d)], sx_recv.at[y], lambda d: {"sp_1": y_at(d)})
    sx_recv[y] = sx_send[y]
    loads["up"].wait()
    loads["dn"].wait()
    up_y()
    dn_y(0)
    dn_z(1)
    arrived(("st1",), first(sx_recv, NY - 1))

    group_state, group_log = block_log(sx_recv[0])
    for p in range(1, NY):
        more, log = block_log(sx_recv[p])
        group_state = jnp.exp(log) * group_state + more
        group_log = group_log + log
    zx_send[...] = with_log(group_state, group_log)
    scatter(
        "st2", NZ, lambda d: zx_send, zx_recv.at[z], lambda d: {"sp_0": lax.rem(z + d, NZ)}
    )
    zx_recv[z] = zx_send[...]
    up_y_half()
    dn_y(1)
    dn_z(2)
    arrived(("st2",), first(zx_recv, NZ - 1))

    run = jnp.zeros((QV, KC), F32)
    for e in range(NZ):
        more, log = block_log(zx_recv[e])
        run = jnp.where(e < z, jnp.exp(log) * run + more, run)
    for p in range(NY):
        px_send[p] = run.astype(BF16)
        more, log = block_log(sx_recv[p])
        run = jnp.exp(log) * run + more
    scatter("st3", NY, lambda d: px_send.at[y_at(d)], px_recv.at[y], lambda d: {"sp_1": y_at(d)})
    px_recv[y] = px_send[y]

    dn_y(7)
    dn_y_half(0)
    up_z(1, 0)
    loads["q"].wait()
    loads["g"].wait()
    loads["ow"].wait()
    loads["hg"].wait()

    def gate_rows_of(n, carry):
        rows = pl.ds(pl.multiple_of(n * 256, 256), 256)
        gate = g_v[rows, :].astype(F32)
        gate_v[rows, :] = hg_ref[...] * (gate / (1.0 + jnp.exp(-gate)))
        return carry

    lax.fori_loop(0, ROWS // 256, gate_rows_of, 0)
    arrived(("st3",), first(px_recv, NY - 1))

    def attend(j):
        s_in = px_recv[...].astype(F32).reshape(DV, KC)
        base = lax.rem(x + j, NX) * 4
        outs = []
        for half in range(2):
            first = base + (1 - c if half == 0 else c) * 2
            for b in range(2):
                n = first + b
                rows = pl.ds(pl.multiple_of(n * BLOCK, BLOCK), BLOCK)
                full = sloc[n] + jnp.exp(cl[n][0:1]) * s_in
                f_hi, f_lo = _split(full)
                qq = q_v[rows, :]
                read = _dot(
                    jnp.concatenate([qq, qq], axis=1),
                    jnp.concatenate([f_hi, f_lo], axis=1),
                    (((1,), (1,)), ((), ())),
                ) * (KC**-0.5)
                scaled = read * lax.rsqrt(jnp.mean(read * read, axis=-1, keepdims=True) + EPS)
                outs.append((scaled * gate_v[rows, :]).astype(BF16))
        heads = jnp.concatenate(outs, axis=0)
        for n in range(4):
            cols = slice(n * 512, (n + 1) * 512)
            part = _dot(heads, ow_v[:, cols])
            psend[0, SLOT[j], :, cols] = part[:OWN].astype(BF16)
            pown[SLOT[j], :, cols] = part[OWN:]
        for name, rows in pair_parts(j):
            send(("dd0", name), psend.at[0, SLOT[j], rows], precv.at[0, SLOT[j], rows], sib)

    def views(rs, n):
        r0, nr, c0, nc = CHUNKS[rs][n]
        return pl.ds(r0, nr), pl.ds(c0, nc), pl.ds(r0 // 2, nr // 2), nr // 2, r0

    def pair_parts(j):
        if j == 2:
            return (((2, 0), pl.ds(0, QR)), ((2, 1), pl.ds(QR, OWN - QR)))
        return ((j, pl.ds(0, OWN)),)

    def pair_sum(rs, j, n):
        rows, cols, _, _, _ = views(rs, n)
        if rs == 0:
            name, part = pair_parts(j)[1 if j == 2 and n > 0 else 0]
            arrived(("dd0", name), precv.at[0, SLOT[j], part])
        elif j == 2:
            arrived(("dd1", 0, n), precv.at[1, 0, rows, cols])
        else:
            arrived(("dd1", 1, n), precv.at[1, pl.ds(1, 3), rows, cols])
        return pown[SLOT[j], rows, cols] + precv[rs, SLOT[j], rows, cols].astype(F32)

    def ring_1(rs, n):
        rows, cols, half, h2, r0 = views(rs, n)
        cs[rs, 0, rows, cols] = pair_sum(rs, 2, n).astype(BF16)
        for d in range(2):
            send(
                (("rx", rs, 1), n),
                cs.at[rs, 0, pl.ds(r0 + d * h2, h2), cols],
                r1.at[rs, d, half, cols],
                x_to[d],
            )

    def ring_2(rs, n):
        rows, cols, half, h2, _ = views(rs, n)
        both = [pair_sum(rs, 1, n), pair_sum(rs, 3, n)]
        arrived((("rx", rs, 1), n), r1.at[rs, :, half, cols])
        for d in range(2):
            more = r1[rs, d, half, cols].astype(F32)
            if d == 0:
                total = jnp.concatenate([both[d][:h2] + more, both[d][h2:]], axis=0)
            else:
                total = jnp.concatenate([both[d][:h2], both[d][h2:] + more], axis=0)
            cs[rs, 1 + d, rows, cols] = total.astype(BF16)
            send((("rx", rs, 2), n), cs.at[rs, 1 + d, rows, cols], r2.at[rs, d, rows, cols], x_to[d])

    def ring_end(rs, n):
        rows, cols, _, _, _ = views(rs, n)
        total = pair_sum(rs, 0, n)
        arrived((("rx", rs, 2), n), r2.at[rs, :, rows, cols])
        return total + r2[rs, 0, rows, cols].astype(F32) + r2[rs, 1, rows, cols].astype(F32)

    def rows_of(q):
        return pl.ds(q * QR, QR)

    def norm_rows(q):
        rows = rows_of(q)
        mid = (stream_v[rows, :].astype(F32) + ring_end(0, q)).astype(BF16)
        mid_v[rows, :] = mid
        midf = mid.astype(F32)
        nrm[1, 0, rows, :] = (
            midf * lax.rsqrt(jnp.mean(midf * midf, axis=-1, keepdims=True) + EPS) * mg_ref[...]
        ).astype(BF16)

    def spread_rows(q):
        rows = rows_of(q)
        for d in range(2):
            send(("ag", q), nrm.at[1, 0, rows], nrm.at[1, 3 if d == 0 else 1, rows], x_to[d])
        send(("ags", q), nrm.at[1, 0, rows], nrm.at[0, 0, rows], sib)

    def spread_mid(q):
        rows = rows_of(q)
        arrived(("ag", q), nrm.at[1, pl.ds(0, 2), rows])
        for d in range(2):
            j = 3 if d == 0 else 1
            part = pl.ds(q * QR + d * (QR // 2), QR // 2)
            send(("agh", q), nrm.at[1, j, part], nrm.at[1, 2, part], x_to[d])
            send(("ags", q), nrm.at[1, j, rows], nrm.at[0, j, rows], sib)

    def spread_end(q):
        rows = rows_of(q)
        arrived(("agh", q), nrm.at[1, 2, rows])
        send(("ags", q), nrm.at[1, 2, rows], nrm.at[0, 2, rows], sib)

    def spread_done(q):
        arrived(("ags", q), nrm.at[0, :, rows_of(q)])

    def ff_up(q, half):
        x_in = nrm[:, :, rows_of(q)].reshape(8 * QR, D)
        for c0 in range(half * (HID // 2), (half + 1) * (HID // 2), 256):
            pre = _dot(x_in, w[:, :, c0 : c0 + 256].reshape(D, 256))
            pre = jnp.maximum(pre, 0.0)
            hid_v[:, c0 : c0 + 256] = (pre * pre).astype(BF16)

    def ff_down(q, g):
        n = G * q + g
        rows, cols, _, _, _ = views(1, n)
        for c0 in range(g * (D // G), (g + 1) * (D // G), 256):
            part = _dot(hid_v[...], wt[:, c0 : c0 + 256]).reshape(2, 4, QR, 256)
            for j in range(4):
                psend[1, SLOT[j], rows, c0 : c0 + 256] = part[0, j].astype(BF16)
                pown[SLOT[j], rows, c0 : c0 + 256] = part[1, j]
        for i, slots in enumerate((pl.ds(0, 1), pl.ds(1, 3))):
            send(("dd1", i, n), psend.at[1, slots, rows, cols], precv.at[1, slots, rows, cols], sib)

    def out_rows(n):
        rows, cols, _, _, _ = views(1, n)
        out_ref[rows, cols] = (mid_v[rows, cols].astype(F32) + ring_end(1, n)).astype(BF16)

    attend(2)
    attend(1)
    dn_z(3)
    dn_y(2)
    dn_y(6)
    up_z(1, 1)
    ring_1(0, 0)
    ring_1(0, 1)
    ring_1(0, 2)
    ring_1(0, 3)
    attend(3)
    attend(0)
    dn_y_half(1)
    dn_y_half(7)
    up_z(2, 0)
    ring_2(0, 0)
    ring_2(0, 1)
    ring_2(0, 2)
    dn_z(4)
    dn_y(3)
    dn_y(5)
    ring_2(0, 3)
    dn_y_half(2)
    dn_y_half(6)
    up_z(2, 1)
    loads["stream"].wait()
    loads["mg"].wait()
    norm_rows(0)
    spread_rows(0)
    dn_turn(0)
    norm_rows(1)
    spread_rows(1)
    up_z(3, 0)
    dn_y(4)
    norm_rows(2)
    dn_turn(1)
    dn_turn(7)
    up_z(3, 1)
    norm_rows(3)
    spread_mid(0)
    spread_rows(2)
    up_z(4, 0)
    dn_y_half(3)
    dn_y_half(5)
    spread_mid(1)
    spread_rows(3)
    dn_turn(2)
    dn_turn(6)
    spread_end(0)
    dn_y_half(4)
    up_z(4, 1)
    spread_mid(2)
    dn_turn(3)
    dn_turn(5)
    up_done()
    spread_done(0)
    ff_up(0, 0)
    spread_end(1)
    dn_turn(4)
    ff_up(0, 1)
    ff_down(0, 0)
    ff_down(0, 1)
    spread_done(1)
    ff_up(1, 0)
    spread_mid(3)
    ring_1(1, 0)
    ff_up(1, 1)
    ring_1(1, 1)
    spread_end(2)
    ff_down(1, 0)
    ff_down(1, 1)
    spread_done(2)
    ff_up(2, 0)
    ring_1(1, 2)
    spread_end(3)
    ff_up(2, 1)
    ring_1(1, 3)
    ring_2(1, 0)
    ff_down(2, 0)
    ring_2(1, 1)
    ff_down(2, 1)
    spread_done(3)
    ff_up(3, 0)
    ring_1(1, 4)
    ring_2(1, 2)
    ff_up(3, 1)
    ring_1(1, 5)
    ff_down(3, 0)
    ring_2(1, 3)
    ff_down(3, 1)
    ring_2(1, 4)
    ring_1(1, 6)
    ring_1(1, 7)
    ring_2(1, 5)
    out_rows(0)
    ring_2(1, 6)
    ring_2(1, 7)
    out_rows(1)
    out_rows(2)
    out_rows(3)
    out_rows(4)
    out_rows(5)
    out_rows(6)
    out_rows(7)

    for family, size in (
        ("ay", some_a(2)),
        ("ayh", some_a(1)),
        ("az", some_a(28)),
        ("bz", some_b(7)),
        ("by", some_b(16)),
        ("byh", some_b(8)),
        ("st1", first(sx_send, NY - 1)),
        ("st2", first(zx_recv, NZ - 1)),
        ("st3", first(px_send, NY - 1)),
        ("dd0", psend.at[0]),
        ("dd1", psend.at[1]),
        (("rx", 0, 1), cs.at[0, 0]),
        (("rx", 0, 2), cs.at[0, pl.ds(1, 2)]),
        (("rx", 1, 1), cs.at[1, 0]),
        (("rx", 1, 2), cs.at[1, pl.ds(1, 2)]),
        ("ag", nrm.at[1, pl.ds(0, 2)]),
        ("agh", nrm.at[1, 0]),
        ("ags", nrm.at[0]),
    ):
        sent(family, size)


def local(
    stream,
    query_rows,
    key_rows,
    value_rows,
    gate_rows,
    log_decay,
    head_gain,
    out_weight,
    mix_gain,
    up_weight,
    down_weight,
):
    any_spec = pl.BlockSpec(memory_space=pl.ANY)
    vmem = pl.BlockSpec(memory_space=pltpu.VMEM)
    return pl.pallas_call(
        kernel,
        out_shape=pltpu.VMEM((OWN, D), BF16),
        in_specs=[any_spec] * 11,
        out_specs=vmem,
        scratch_shapes=[
            pltpu.VMEM((1, DV), F32),
            pltpu.VMEM((1, D), F32),
            pltpu.VMEM((OWN, D), BF16),
            pltpu.VMEM((ROWS, KC), BF16),
            pltpu.VMEM((ROWS, KC), BF16),
            pltpu.VMEM((ROWS, DV), BF16),
            pltpu.VMEM((ROWS, DV), BF16),
            pltpu.VMEM((ROWS, DV), F32),
            pltpu.VMEM((ROWS, KC), F32),
            pltpu.VMEM((DV, D), BF16),
            pltpu.VMEM((NSP, WR, 2 * HID), BF16),
            pltpu.VMEM((HID, D), BF16),
            pltpu.VMEM((NB, DV, KC), F32),
            pltpu.VMEM((NB, 8, KC), F32),
            pltpu.VMEM((NY, DV // NY + 16, KC), BF16),
            pltpu.VMEM((NY, DV // NY + 16, KC), BF16),
            pltpu.VMEM((DV // NY + 16, KC), BF16),
            pltpu.VMEM((NZ, DV // NY + 16, KC), BF16),
            pltpu.VMEM((NY, DV // NY, KC), BF16),
            pltpu.VMEM((NY, DV // NY, KC), BF16),
            pltpu.VMEM((2, 4, OWN, D), BF16),
            pltpu.VMEM((2, 4, OWN, D), BF16),
            pltpu.VMEM((4, OWN, D), F32),
            pltpu.VMEM((2, 3, OWN, D), BF16),
            pltpu.VMEM((2, 2, OWN // 2, D), BF16),
            pltpu.VMEM((2, 2, OWN, D), BF16),
            pltpu.VMEM((2, 4, OWN, D), BF16),
            pltpu.VMEM((OWN, D), BF16),
            pltpu.VMEM((8 * QR, HID), BF16),
            pltpu.SemaphoreType.DMA((11,)),
            pltpu.SemaphoreType.DMA((len(SEND),)),
            pltpu.SemaphoreType.DMA((len(RECV),)),
        ],
        compiler_params=pltpu.CompilerParams(
            collective_id=0, has_side_effects=True, vmem_limit_bytes=60 * 1024 * 1024
        ),
        name="layer",
    )(
        stream,
        query_rows,
        key_rows,
        value_rows,
        gate_rows,
        log_decay,
        head_gain.reshape(1, DV),
        out_weight,
        mix_gain.reshape(1, D),
        up_weight,
        down_weight,
    )


def solution(mesh):
    torus = Mesh(mesh.devices.reshape(NZ, NY, NX, 2), SP_TP)
    in_specs = (
        P(SP_TP, None),
        P(SP, TP),
        P(SP, TP),
        P(SP, TP),
        P(SP, TP),
        P(SP, TP),
        P(),
        P(TP, None),
        P(),
        P(SP, TP),
        P(SP, TP),
    )
    out_specs = P(SP_TP, None)
    return jax.shard_map(local, mesh=torus, in_specs=in_specs, out_specs=out_specs, check_vma=False)
```

```python
import functools

import jax
import jax.numpy as jnp
from jax import lax
from jax.experimental import pallas as pl
from jax.experimental.pallas import tpu as pltpu
from jax.sharding import Mesh
from jax.sharding import PartitionSpec as P

KC = 128
DV = 256
BLOCK = 64
D = 2048
ROWS = 1024
OWN = 128
NB = ROWS // BLOCK
NZ, NY, NX = 8, 4, 4
NSP = NZ * NY
Q = 4
QR = OWN // Q
HID = 1024
WR = 64
AC = 768
EPS = 1e-06
SP = ("sp_0", "sp_1")
TP = ("tp_0", "tp_1")
SP_TP = ("sp_0", "sp_1", "tp_0", "tp_1")
MESH = pl.DeviceIdType.MESH
F32 = jnp.float32
BF16 = jnp.bfloat16

G = 2
CH1 = tuple((q * QR, QR, 0, D) for q in range(Q))
CH2 = tuple((q * QR, QR, g * (D // G), D // G) for q in range(Q) for g in range(G))
CHUNKS = (CH1, CH2)
SLOT = {2: 0, 1: 1, 3: 2, 0: 3}

RECV, SEND = {}, {}


def _recv_id(*name):
    RECV.setdefault(name, len(RECV))
    SEND.setdefault(name[0], len(SEND))


for _n in ("ay", "ayh", "st1", "st2", "st3"):
    _recv_id(_n)
for _i in (1, 2, 3, 4):
    _recv_id("bz", _i)
    for _h in range(2 if _i < 4 else 1):
        _recv_id("az", _i, _h)
for _k in range(8):
    _recv_id("by", _k)
    _recv_id("byh", _k)
for _n in ((2, 0), (2, 1), 1, 3, 0):
    _recv_id("dd0", _n)
for _n in range(len(CH2)):
    _recv_id("dd1", 0, _n)
    _recv_id("dd1", 1, _n)
for _rs in range(2):
    for _n in range(len(CHUNKS[_rs])):
        for _s in (1, 2):
            _recv_id(("rx", _rs, _s), _n)
for _q in range(Q):
    _recv_id("ag", _q)
    _recv_id("agh", _q)
    _recv_id("ags", _q)


def _dot(a, b, dims=(((1,), (0,)), ((), ()))):
    return lax.dot_general(a, b, dims, preferred_element_type=F32)


def _split(x):
    hi = x.astype(BF16)
    return hi, (x - hi.astype(F32)).astype(BF16)


def kernel(
    stream_h,
    q_h,
    k_h,
    v_h,
    g_h,
    ld_h,
    hg_h,
    ow_h,
    mg_h,
    up_h,
    dn_h,
    out_ref,
    hg_ref,
    mg_ref,
    stream_v,
    q_v,
    k_v,
    v_v,
    g_v,
    gate_v,
    ld_v,
    ow_v,
    w,
    wt,
    sloc,
    cl,
    sx_send,
    sx_recv,
    zx_send,
    zx_recv,
    px_send,
    px_recv,
    psend,
    precv,
    pown,
    cs,
    r1,
    r2,
    nrm,
    mid_v,
    hid_v,
    lsem,
    ssem,
    rsem,
):
    z, y = lax.axis_index("sp_0"), lax.axis_index("sp_1")
    x, c = lax.axis_index("tp_0"), lax.axis_index("tp_1")
    sp = z * NY + y
    yl, yr = lax.rem(y + NY - 1, NY), lax.rem(y + 1, NY)
    zl, zr = lax.rem(z + NZ - 1, NZ), lax.rem(z + 1, NZ)
    xl, xr = lax.rem(x + NX - 1, NX), lax.rem(x + 1, NX)
    y_to, y_from = ({"sp_1": yr}, {"sp_1": yl}), (yl, yr)
    z_to = ({"sp_0": zr}, {"sp_0": zl})
    x_to = ({"tp_0": xr}, {"tp_0": xl})
    sib = {"tp_1": 1 - c}

    barrier = pltpu.get_barrier_semaphore()

    def signal_to(other):
        pl.semaphore_signal(barrier, inc=1, device_id=other, device_id_type=MESH)

    def greet_y(d, carry):
        signal_to({"sp_1": lax.rem(y + d, NY)})
        return carry

    def greet_z(d, carry):
        signal_to({"sp_0": lax.rem(z + d, NZ)})
        return carry

    lax.fori_loop(1, NY, greet_y, 0)
    lax.fori_loop(1, NZ, greet_z, 0)
    for other in (x_to[0], x_to[1], sib):
        signal_to(other)

    loads = {}

    def load(name, src, dst, i):
        loads[name] = pltpu.make_async_copy(src, dst, lsem.at[i])
        loads[name].start()

    load("ld", ld_h, ld_v, 0)
    load("k", k_h, k_v, 1)
    load("v", v_h, v_v, 2)

    def send(name, src, dst, to):
        pltpu.make_async_remote_copy(
            src_ref=src,
            dst_ref=dst,
            send_sem=ssem.at[SEND[name[0]]],
            recv_sem=rsem.at[RECV[name]],
            device_id=to,
            device_id_type=MESH,
        ).start()

    waited = set()

    def arrived(name, size):
        if name not in waited:
            waited.add(name)
            pltpu.make_async_copy(size, size, rsem.at[RECV[name]]).wait()

    def sent(family, size):
        pltpu.make_async_copy(size, size, ssem.at[SEND[family]]).wait()

    HALF = (pl.ds(0, WR // 2), pl.ds(WR // 2, WR // 2))
    COLS_A, COLS_B = pl.ds(0, AC), pl.ds(AC, 2 * HID - AC)

    def zat(off):
        return lax.rem(z + off + NZ, NZ)

    def some_a(n):
        return w.at[pl.ds(0, n), :, COLS_A]

    def some_b(n):
        return w.at[pl.ds(0, n), :, COLS_B]

    def up_y():
        for d in range(2):
            part = w.at[sp, :, COLS_A]
            send(("ay",), part, part, y_to[d])

    def up_y_half():
        arrived(("ay",), some_a(2))
        for d in range(2):
            part = w.at[z * NY + y_from[d], HALF[d], COLS_A]
            send(("ayh",), part, part, y_to[d])

    def up_z(i, step):
        if i == 1:
            arrived(("ayh",), some_a(1))
        else:
            arrived(("az", i - 1, step), some_a(4))
        if i < 4 or step == 0:
            for d in range(2):
                zz = zat(-(i - 1) if d == 0 else i - 1)
                part = w.at[pl.ds(zz * NY, NY), HALF[step if d == 0 else 1 - step], COLS_A]
                send(("az", i, step), part, part, z_to[d])

    def up_done():
        arrived(("az", 4, 0), some_a(4))

    def dn_z(i):
        if i > 1:
            arrived(("bz", i - 1), some_b(2))
        for d in range(2):
            blk = zat(-(i - 1) if d == 0 else i - 1) * NY + y
            part = w.at[blk, :, COLS_B] if i < 4 else w.at[blk, HALF[d], COLS_B]
            send(("bz", i), part, part, z_to[d])

    def dn_y(k):
        if k in (1, 7):
            arrived(("bz", 1), some_b(2))
        if k == 4:
            arrived(("bz", 4), some_b(1))
        part = w.at[zat(k) * NY + y, :, COLS_B]
        for d in range(2):
            send(("by", k), part, part, y_to[d])

    def dn_y_half(k):
        arrived(("by", k), some_b(2))
        for d in range(2):
            part = w.at[zat(k) * NY + y_from[d], HALF[d], COLS_B]
            send(("byh", k), part, part, y_to[d])

    def dn_turn(k):
        arrived(("byh", k), some_b(1))
        zz = zat(k)
        slab = w[pl.ds(zz * NY, NY), :, pl.ds(HID, HID)].reshape(NY * WR, HID)
        wt[:, pl.ds(pl.multiple_of(zz * NY * WR, NY * WR), NY * WR)] = slab.T

    loads["ld"].wait()
    loads["k"].wait()
    loads["v"].wait()
    load("up", up_h, w.at[sp, :, pl.ds(0, HID)], 3)
    load("dn", dn_h, w.at[sp, :, pl.ds(HID, HID)], 4)
    load("q", q_h, q_v, 5)
    load("g", g_h, g_v, 6)
    load("ow", ow_h, ow_v, 7)
    load("stream", stream_h, stream_v, 8)
    load("hg", hg_h, hg_ref, 9)
    load("mg", mg_h, mg_ref, 10)
    r_i = lax.broadcasted_iota(jnp.int32, (256, 256), 0)
    c_i = lax.broadcasted_iota(jnp.int32, (256, 256), 1)
    tri = jnp.where((c_i > r_i) & (c_i // BLOCK == r_i // BLOCK), 1.0, 0.0).astype(BF16)

    def group(gi, state, total):
        rows = slice(gi * 256, (gi + 1) * 256)
        ld = ld_v[rows, :]
        hi, lo = _split(ld)
        lo2 = (ld - hi.astype(F32) - lo.astype(F32)).astype(BF16)
        suf = _dot(tri, hi) + _dot(tri, lo) + _dot(tri, lo2)
        dk = k_v[rows, :].astype(F32) * jnp.exp(suf)
        dk_hi, dk_lo = _split(dk)
        vals = v_v[rows, :]
        for b in range(4):
            s = slice(b * BLOCK, (b + 1) * BLOCK)
            vv = jnp.concatenate([vals[s], vals[s]], axis=0)
            dd = jnp.concatenate([dk_hi[s], dk_lo[s]], axis=0)
            upd = _dot(vv, dd, (((0,), (0,)), ((), ())))
            last = suf[b * BLOCK : b * BLOCK + 1] + ld[b * BLOCK : b * BLOCK + 1]
            state = jnp.exp(last) * state + upd
            total = total + last
            sloc[gi * 4 + b] = state
            cl[gi * 4 + b] = jnp.broadcast_to(total, (8, KC))
        return state, total

    state, total = jnp.zeros((DV, KC), F32), jnp.zeros((1, KC), F32)
    for gi in range(NB // 4):
        state, total = group(gi, state, total)

    QV = DV // NY

    def with_log(block, log):
        hi, lo = _split(log)
        lo2 = (log - hi.astype(F32) - lo.astype(F32)).astype(BF16)
        sub = lax.broadcasted_iota(jnp.int32, (16, KC), 0)
        logs = jnp.where(
            sub == 0,
            hi.astype(F32),
            jnp.where(sub == 1, lo.astype(F32), jnp.where(sub == 2, lo2.astype(F32), 0.0)),
        )
        return jnp.concatenate([block, logs], axis=0).astype(BF16)

    def block_log(tile):
        t = tile.astype(F32)
        return t[:QV], t[QV : QV + 1] + t[QV + 1 : QV + 2] + t[QV + 2 : QV + 3]

    def first(ref, count):
        return ref.at[pl.ds(0, count)]

    def scatter(name, count, src_of, dst, to):
        def one(d, carry):
            pltpu.make_async_remote_copy(
                src_ref=src_of(d),
                dst_ref=dst,
                send_sem=ssem.at[SEND[name]],
                recv_sem=rsem.at[RECV[(name,)]],
                device_id=to(d),
                device_id_type=MESH,
            ).start()
            return carry

        lax.fori_loop(1, count, one, 0)

    def y_at(d):
        return lax.rem(y + d, NY)

    for p in range(NY):
        sx_send[p] = with_log(state[p * QV : (p + 1) * QV], total)

    pl.semaphore_wait(barrier, NY - 1 + NZ - 1 + 3)
    scatter("st1", NY, lambda d: sx_send.at[y_at(d)], sx_recv.at[y], lambda d: {"sp_1": y_at(d)})
    sx_recv[y] = sx_send[y]
    loads["up"].wait()
    loads["dn"].wait()
    up_y()
    dn_y(0)
    dn_z(1)
    arrived(("st1",), first(sx_recv, NY - 1))

    group_state, group_log = block_log(sx_recv[0])
    for p in range(1, NY):
        more, log = block_log(sx_recv[p])
        group_state = jnp.exp(log) * group_state + more
        group_log = group_log + log
    zx_send[...] = with_log(group_state, group_log)
    scatter(
        "st2", NZ, lambda d: zx_send, zx_recv.at[z], lambda d: {"sp_0": lax.rem(z + d, NZ)}
    )
    zx_recv[z] = zx_send[...]
    up_y_half()
    dn_y(1)
    dn_z(2)
    arrived(("st2",), first(zx_recv, NZ - 1))

    run = jnp.zeros((QV, KC), F32)
    for e in range(NZ):
        more, log = block_log(zx_recv[e])
        run = jnp.where(e < z, jnp.exp(log) * run + more, run)
    for p in range(NY):
        px_send[p] = run.astype(BF16)
        more, log = block_log(sx_recv[p])
        run = jnp.exp(log) * run + more
    scatter("st3", NY, lambda d: px_send.at[y_at(d)], px_recv.at[y], lambda d: {"sp_1": y_at(d)})
    px_recv[y] = px_send[y]

    dn_y(7)
    dn_y_half(0)
    up_z(1, 0)
    loads["q"].wait()
    loads["g"].wait()
    loads["ow"].wait()
    loads["hg"].wait()

    def gate_rows_of(n, carry):
        rows = pl.ds(pl.multiple_of(n * 256, 256), 256)
        gate = g_v[rows, :].astype(F32)
        gate_v[rows, :] = hg_ref[...] * (gate / (1.0 + jnp.exp(-gate)))
        return carry

    lax.fori_loop(0, ROWS // 256, gate_rows_of, 0)
    dn_z(3)
    dn_y(2)
    dn_y(6)
    up_z(1, 1)
    arrived(("st3",), first(px_recv, NY - 1))

    def attend(j):
        s_in = px_recv[...].astype(F32).reshape(DV, KC)
        base = lax.rem(x + j, NX) * 4
        outs = []
        for half in range(2):
            first = base + (1 - c if half == 0 else c) * 2
            for b in range(2):
                n = first + b
                rows = pl.ds(pl.multiple_of(n * BLOCK, BLOCK), BLOCK)
                full = sloc[n] + jnp.exp(cl[n][0:1]) * s_in
                f_hi, f_lo = _split(full)
                qq = q_v[rows, :]
                read = _dot(
                    jnp.concatenate([qq, qq], axis=1),
                    jnp.concatenate([f_hi, f_lo], axis=1),
                    (((1,), (1,)), ((), ())),
                ) * (KC**-0.5)
                scaled = read * lax.rsqrt(jnp.mean(read * read, axis=-1, keepdims=True) + EPS)
                outs.append((scaled * gate_v[rows, :]).astype(BF16))
        heads = jnp.concatenate(outs, axis=0)
        for n in range(4):
            cols = slice(n * 512, (n + 1) * 512)
            part = _dot(heads, ow_v[:, cols])
            psend[0, SLOT[j], :, cols] = part[:OWN].astype(BF16)
            pown[SLOT[j], :, cols] = part[OWN:]
        for name, rows in pair_parts(j):
            send(("dd0", name), psend.at[0, SLOT[j], rows], precv.at[0, SLOT[j], rows], sib)

    def views(rs, n):
        r0, nr, c0, nc = CHUNKS[rs][n]
        return pl.ds(r0, nr), pl.ds(c0, nc), pl.ds(r0 // 2, nr // 2), nr // 2, r0

    def pair_parts(j):
        if j == 2:
            return (((2, 0), pl.ds(0, QR)), ((2, 1), pl.ds(QR, OWN - QR)))
        return ((j, pl.ds(0, OWN)),)

    def pair_sum(rs, j, n):
        rows, cols, _, _, _ = views(rs, n)
        if rs == 0:
            name, part = pair_parts(j)[1 if j == 2 and n > 0 else 0]
            arrived(("dd0", name), precv.at[0, SLOT[j], part])
        elif j == 2:
            arrived(("dd1", 0, n), precv.at[1, 0, rows, cols])
        else:
            arrived(("dd1", 1, n), precv.at[1, pl.ds(1, 3), rows, cols])
        return pown[SLOT[j], rows, cols] + precv[rs, SLOT[j], rows, cols].astype(F32)

    def ring_1(rs, n):
        rows, cols, half, h2, r0 = views(rs, n)
        cs[rs, 0, rows, cols] = pair_sum(rs, 2, n).astype(BF16)
        for d in range(2):
            send(
                (("rx", rs, 1), n),
                cs.at[rs, 0, pl.ds(r0 + d * h2, h2), cols],
                r1.at[rs, d, half, cols],
                x_to[d],
            )

    def ring_2(rs, n):
        rows, cols, half, h2, _ = views(rs, n)
        both = [pair_sum(rs, 1, n), pair_sum(rs, 3, n)]
        arrived((("rx", rs, 1), n), r1.at[rs, :, half, cols])
        for d in range(2):
            more = r1[rs, d, half, cols].astype(F32)
            if d == 0:
                total = jnp.concatenate([both[d][:h2] + more, both[d][h2:]], axis=0)
            else:
                total = jnp.concatenate([both[d][:h2], both[d][h2:] + more], axis=0)
            cs[rs, 1 + d, rows, cols] = total.astype(BF16)
            send((("rx", rs, 2), n), cs.at[rs, 1 + d, rows, cols], r2.at[rs, d, rows, cols], x_to[d])

    def ring_end(rs, n):
        rows, cols, _, _, _ = views(rs, n)
        total = pair_sum(rs, 0, n)
        arrived((("rx", rs, 2), n), r2.at[rs, :, rows, cols])
        return total + r2[rs, 0, rows, cols].astype(F32) + r2[rs, 1, rows, cols].astype(F32)

    def rows_of(q):
        return pl.ds(q * QR, QR)

    def norm_rows(q):
        rows = rows_of(q)
        mid = (stream_v[rows, :].astype(F32) + ring_end(0, q)).astype(BF16)
        mid_v[rows, :] = mid
        midf = mid.astype(F32)
        nrm[1, 0, rows, :] = (
            midf * lax.rsqrt(jnp.mean(midf * midf, axis=-1, keepdims=True) + EPS) * mg_ref[...]
        ).astype(BF16)

    def spread_rows(q):
        rows = rows_of(q)
        for d in range(2):
            send(("ag", q), nrm.at[1, 0, rows], nrm.at[1, 3 if d == 0 else 1, rows], x_to[d])
        send(("ags", q), nrm.at[1, 0, rows], nrm.at[0, 0, rows], sib)

    def spread_mid(q):
        rows = rows_of(q)
        arrived(("ag", q), nrm.at[1, pl.ds(0, 2), rows])
        for d in range(2):
            j = 3 if d == 0 else 1
            part = pl.ds(q * QR + d * (QR // 2), QR // 2)
            send(("agh", q), nrm.at[1, j, part], nrm.at[1, 2, part], x_to[d])
            send(("ags", q), nrm.at[1, j, rows], nrm.at[0, j, rows], sib)

    def spread_end(q):
        rows = rows_of(q)
        arrived(("agh", q), nrm.at[1, 2, rows])
        send(("ags", q), nrm.at[1, 2, rows], nrm.at[0, 2, rows], sib)

    def spread_done(q):
        arrived(("ags", q), nrm.at[0, :, rows_of(q)])

    def ff_up(q, half):
        x_in = nrm[:, :, rows_of(q)].reshape(8 * QR, D)
        for c0 in range(half * (HID // 2), (half + 1) * (HID // 2), 256):
            pre = _dot(x_in, w[:, :, c0 : c0 + 256].reshape(D, 256))
            pre = jnp.maximum(pre, 0.0)
            hid_v[:, c0 : c0 + 256] = (pre * pre).astype(BF16)

    def ff_down(q, g):
        n = G * q + g
        rows, cols, _, _, _ = views(1, n)
        for c0 in range(g * (D // G), (g + 1) * (D // G), 256):
            part = _dot(hid_v[...], wt[:, c0 : c0 + 256]).reshape(2, 4, QR, 256)
            for j in range(4):
                psend[1, SLOT[j], rows, c0 : c0 + 256] = part[0, j].astype(BF16)
                pown[SLOT[j], rows, c0 : c0 + 256] = part[1, j]
        for i, slots in enumerate((pl.ds(0, 1), pl.ds(1, 3))):
            send(("dd1", i, n), psend.at[1, slots, rows, cols], precv.at[1, slots, rows, cols], sib)

    def out_rows(n):
        rows, cols, _, _, _ = views(1, n)
        out_ref[rows, cols] = (mid_v[rows, cols].astype(F32) + ring_end(1, n)).astype(BF16)

    attend(2)
    attend(1)
    ring_1(0, 0)
    ring_1(0, 1)
    ring_1(0, 2)
    ring_1(0, 3)
    attend(3)
    attend(0)
    dn_y_half(1)
    dn_y_half(7)
    up_z(2, 0)
    ring_2(0, 0)
    ring_2(0, 1)
    ring_2(0, 2)
    dn_z(4)
    dn_y(3)
    dn_y(5)
    ring_2(0, 3)
    dn_y_half(2)
    dn_y_half(6)
    up_z(2, 1)
    loads["stream"].wait()
    loads["mg"].wait()
    norm_rows(0)
    spread_rows(0)
    dn_turn(0)
    norm_rows(1)
    spread_rows(1)
    up_z(3, 0)
    dn_y(4)
    norm_rows(2)
    dn_turn(1)
    dn_turn(7)
    up_z(3, 1)
    norm_rows(3)
    spread_mid(0)
    spread_rows(2)
    up_z(4, 0)
    dn_y_half(3)
    dn_y_half(5)
    spread_mid(1)
    spread_rows(3)
    dn_turn(2)
    dn_turn(6)
    spread_end(0)
    dn_y_half(4)
    up_z(4, 1)
    spread_mid(2)
    up_done()
    spread_done(0)
    ff_up(0, 0)
    dn_turn(3)
    dn_turn(5)
    spread_end(1)
    dn_turn(4)
    ff_up(0, 1)
    ff_down(0, 0)
    ff_down(0, 1)
    spread_done(1)
    ff_up(1, 0)
    spread_mid(3)
    ring_1(1, 0)
    ff_up(1, 1)
    ring_1(1, 1)
    spread_end(2)
    ff_down(1, 0)
    ff_down(1, 1)
    spread_done(2)
    ff_up(2, 0)
    ring_1(1, 2)
    ff_up(2, 1)
    ring_1(1, 3)
    spread_end(3)
    ring_2(1, 0)
    ff_down(2, 0)
    ff_down(2, 1)
    ring_2(1, 1)
    spread_done(3)
    ff_up(3, 0)
    ring_1(1, 4)
    ring_2(1, 2)
    ff_up(3, 1)
    ring_1(1, 5)
    ff_down(3, 0)
    ring_2(1, 3)
    ff_down(3, 1)
    ring_2(1, 4)
    ring_1(1, 6)
    ring_1(1, 7)
    ring_2(1, 5)
    out_rows(0)
    ring_2(1, 6)
    ring_2(1, 7)
    out_rows(1)
    out_rows(2)
    out_rows(3)
    out_rows(4)
    out_rows(5)
    out_rows(6)
    out_rows(7)

    for family, size in (
        ("ay", some_a(2)),
        ("ayh", some_a(1)),
        ("az", some_a(28)),
        ("bz", some_b(7)),
        ("by", some_b(16)),
        ("byh", some_b(8)),
        ("st1", first(sx_send, NY - 1)),
        ("st2", first(zx_recv, NZ - 1)),
        ("st3", first(px_send, NY - 1)),
        ("dd0", psend.at[0]),
        ("dd1", psend.at[1]),
        (("rx", 0, 1), cs.at[0, 0]),
        (("rx", 0, 2), cs.at[0, pl.ds(1, 2)]),
        (("rx", 1, 1), cs.at[1, 0]),
        (("rx", 1, 2), cs.at[1, pl.ds(1, 2)]),
        ("ag", nrm.at[1, pl.ds(0, 2)]),
        ("agh", nrm.at[1, 0]),
        ("ags", nrm.at[0]),
    ):
        sent(family, size)


def local(
    stream,
    query_rows,
    key_rows,
    value_rows,
    gate_rows,
    log_decay,
    head_gain,
    out_weight,
    mix_gain,
    up_weight,
    down_weight,
):
    any_spec = pl.BlockSpec(memory_space=pl.ANY)
    vmem = pl.BlockSpec(memory_space=pltpu.VMEM)
    return pl.pallas_call(
        kernel,
        out_shape=pltpu.VMEM((OWN, D), BF16),
        in_specs=[any_spec] * 11,
        out_specs=vmem,
        scratch_shapes=[
            pltpu.VMEM((1, DV), F32),
            pltpu.VMEM((1, D), F32),
            pltpu.VMEM((OWN, D), BF16),
            pltpu.VMEM((ROWS, KC), BF16),
            pltpu.VMEM((ROWS, KC), BF16),
            pltpu.VMEM((ROWS, DV), BF16),
            pltpu.VMEM((ROWS, DV), BF16),
            pltpu.VMEM((ROWS, DV), F32),
            pltpu.VMEM((ROWS, KC), F32),
            pltpu.VMEM((DV, D), BF16),
            pltpu.VMEM((NSP, WR, 2 * HID), BF16),
            pltpu.VMEM((HID, D), BF16),
            pltpu.VMEM((NB, DV, KC), F32),
            pltpu.VMEM((NB, 8, KC), F32),
            pltpu.VMEM((NY, DV // NY + 16, KC), BF16),
            pltpu.VMEM((NY, DV // NY + 16, KC), BF16),
            pltpu.VMEM((DV // NY + 16, KC), BF16),
            pltpu.VMEM((NZ, DV // NY + 16, KC), BF16),
            pltpu.VMEM((NY, DV // NY, KC), BF16),
            pltpu.VMEM((NY, DV // NY, KC), BF16),
            pltpu.VMEM((2, 4, OWN, D), BF16),
            pltpu.VMEM((2, 4, OWN, D), BF16),
            pltpu.VMEM((4, OWN, D), F32),
            pltpu.VMEM((2, 3, OWN, D), BF16),
            pltpu.VMEM((2, 2, OWN // 2, D), BF16),
            pltpu.VMEM((2, 2, OWN, D), BF16),
            pltpu.VMEM((2, 4, OWN, D), BF16),
            pltpu.VMEM((OWN, D), BF16),
            pltpu.VMEM((8 * QR, HID), BF16),
            pltpu.SemaphoreType.DMA((11,)),
            pltpu.SemaphoreType.DMA((len(SEND),)),
            pltpu.SemaphoreType.DMA((len(RECV),)),
        ],
        compiler_params=pltpu.CompilerParams(
            collective_id=0, has_side_effects=True, vmem_limit_bytes=60 * 1024 * 1024
        ),
        name="layer",
    )(
        stream,
        query_rows,
        key_rows,
        value_rows,
        gate_rows,
        log_decay,
        head_gain.reshape(1, DV),
        out_weight,
        mix_gain.reshape(1, D),
        up_weight,
        down_weight,
    )


def solution(mesh):
    torus = Mesh(mesh.devices.reshape(NZ, NY, NX, 2), SP_TP)
    in_specs = (
        P(SP_TP, None),
        P(SP, TP),
        P(SP, TP),
        P(SP, TP),
        P(SP, TP),
        P(SP, TP),
        P(),
        P(TP, None),
        P(),
        P(SP, TP),
        P(SP, TP),
    )
    out_specs = P(SP_TP, None)
    return jax.shard_map(local, mesh=torus, in_specs=in_specs, out_specs=out_specs, check_vma=False)
```

```python
import functools

import jax
import jax.numpy as jnp
from jax import lax
from jax.experimental import pallas as pl
from jax.experimental.pallas import tpu as pltpu
from jax.sharding import Mesh
from jax.sharding import PartitionSpec as P

KC = 128
DV = 256
BLOCK = 64
D = 2048
ROWS = 1024
OWN = 128
NB = ROWS // BLOCK
NZ, NY, NX = 8, 4, 4
NSP = NZ * NY
Q = 4
QR = OWN // Q
HID = 1024
WR = 64
AC = 768
EPS = 1e-06
SP = ("sp_0", "sp_1")
TP = ("tp_0", "tp_1")
SP_TP = ("sp_0", "sp_1", "tp_0", "tp_1")
MESH = pl.DeviceIdType.MESH
F32 = jnp.float32
BF16 = jnp.bfloat16

G = 2
CH1 = tuple((q * QR, QR, 0, D) for q in range(Q))
CH2 = tuple((q * QR, QR, g * (D // G), D // G) for q in range(Q) for g in range(G))
CHUNKS = (CH1, CH2)
SLOT = {2: 0, 1: 1, 3: 2, 0: 3}

RECV, SEND = {}, {}
FAMILY = {"ay": "az", "ayh": "az", "by": "bz", "byh": "bz", "dd1": "dd0"}


def _family(first):
    return "rx" if isinstance(first, tuple) else FAMILY.get(first, first)


def _recv_id(*name):
    RECV.setdefault(name, len(RECV))
    SEND.setdefault(_family(name[0]), len(SEND))


for _n in ("ay", "ayh", "st1", "st2", "st3"):
    _recv_id(_n)
for _i in (1, 2, 3, 4):
    _recv_id("bz", _i)
    for _h in range(2 if _i < 4 else 1):
        _recv_id("az", _i, _h)
for _k in range(8):
    _recv_id("by", _k)
    _recv_id("byh", _k)
for _n in ((2, 0), (2, 1), 1, 3, 0):
    _recv_id("dd0", _n)
for _n in range(len(CH2)):
    _recv_id("dd1", 0, _n)
    _recv_id("dd1", 1, _n)
for _rs in range(2):
    for _n in range(len(CHUNKS[_rs])):
        for _s in (1, 2):
            _recv_id(("rx", _rs, _s), _n)
for _q in range(Q):
    _recv_id("ag", _q)
    _recv_id("agh", _q)
    _recv_id("ags", _q)


def _dot(a, b, dims=(((1,), (0,)), ((), ()))):
    return lax.dot_general(a, b, dims, preferred_element_type=F32)


def _split(x):
    hi = x.astype(BF16)
    return hi, (x - hi.astype(F32)).astype(BF16)


def kernel(
    stream_h,
    q_h,
    k_h,
    v_h,
    g_h,
    ld_h,
    hg_h,
    ow_h,
    mg_h,
    up_h,
    dn_h,
    out_ref,
    hg_ref,
    mg_ref,
    stream_v,
    q_v,
    k_v,
    v_v,
    g_v,
    gate_v,
    ld_v,
    ow_v,
    w,
    wt,
    sloc,
    cl,
    sx_send,
    sx_recv,
    zx_send,
    zx_recv,
    px_send,
    px_recv,
    psend,
    precv,
    pown,
    cs,
    r1,
    r2,
    nrm,
    mid_v,
    hid_v,
    lsem,
    ssem,
    rsem,
):
    z, y = lax.axis_index("sp_0"), lax.axis_index("sp_1")
    x, c = lax.axis_index("tp_0"), lax.axis_index("tp_1")
    sp = z * NY + y
    yl, yr = lax.rem(y + NY - 1, NY), lax.rem(y + 1, NY)
    zl, zr = lax.rem(z + NZ - 1, NZ), lax.rem(z + 1, NZ)
    xl, xr = lax.rem(x + NX - 1, NX), lax.rem(x + 1, NX)
    y_to, y_from = ({"sp_1": yr}, {"sp_1": yl}), (yl, yr)
    z_to = ({"sp_0": zr}, {"sp_0": zl})
    x_to = ({"tp_0": xr}, {"tp_0": xl})
    sib = {"tp_1": 1 - c}

    barrier = pltpu.get_barrier_semaphore()

    def signal_to(other):
        pl.semaphore_signal(barrier, inc=1, device_id=other, device_id_type=MESH)

    def greet_y(d, carry):
        signal_to({"sp_1": lax.rem(y + d, NY)})
        return carry

    def greet_z(d, carry):
        signal_to({"sp_0": lax.rem(z + d, NZ)})
        return carry

    lax.fori_loop(1, NY, greet_y, 0)
    lax.fori_loop(1, NZ, greet_z, 0)
    for other in (x_to[0], x_to[1], sib):
        signal_to(other)

    loads = {}

    def load(name, src, dst, i):
        loads[name] = pltpu.make_async_copy(src, dst, lsem.at[i])
        loads[name].start()

    load("ld", ld_h, ld_v, 0)
    load("k", k_h, k_v, 1)
    load("v", v_h, v_v, 2)

    def send(name, src, dst, to):
        pltpu.make_async_remote_copy(
            src_ref=src,
            dst_ref=dst,
            send_sem=ssem.at[SEND[_family(name[0])]],
            recv_sem=rsem.at[RECV[name]],
            device_id=to,
            device_id_type=MESH,
        ).start()

    waited = set()

    def arrived(name, size):
        if name not in waited:
            waited.add(name)
            pltpu.make_async_copy(size, size, rsem.at[RECV[name]]).wait()

    def sent(family, size):
        pltpu.make_async_copy(size, size, ssem.at[SEND[family]]).wait()

    HALF = (pl.ds(0, WR // 2), pl.ds(WR // 2, WR // 2))
    COLS_A, COLS_B = pl.ds(0, AC), pl.ds(AC, 2 * HID - AC)

    def zat(off):
        return lax.rem(z + off + NZ, NZ)

    def some_a(n):
        return w.at[pl.ds(0, n), :, COLS_A]

    def some_b(n):
        return w.at[pl.ds(0, n), :, COLS_B]

    def up_y():
        for d in range(2):
            part = w.at[sp, :, COLS_A]
            send(("ay",), part, part, y_to[d])

    def up_y_half():
        arrived(("ay",), some_a(2))
        for d in range(2):
            part = w.at[z * NY + y_from[d], HALF[d], COLS_A]
            send(("ayh",), part, part, y_to[d])

    def up_z(i, step):
        if i == 1:
            arrived(("ayh",), some_a(1))
        else:
            arrived(("az", i - 1, step), some_a(4))
        if i < 4 or step == 0:
            for d in range(2):
                zz = zat(-(i - 1) if d == 0 else i - 1)
                part = w.at[pl.ds(zz * NY, NY), HALF[step if d == 0 else 1 - step], COLS_A]
                send(("az", i, step), part, part, z_to[d])

    def up_done():
        arrived(("az", 4, 0), some_a(4))

    def dn_z(i):
        if i > 1:
            arrived(("bz", i - 1), some_b(2))
        for d in range(2):
            blk = zat(-(i - 1) if d == 0 else i - 1) * NY + y
            part = w.at[blk, :, COLS_B] if i < 4 else w.at[blk, HALF[d], COLS_B]
            send(("bz", i), part, part, z_to[d])

    def dn_y(k):
        if k in (1, 7):
            arrived(("bz", 1), some_b(2))
        if k == 4:
            arrived(("bz", 4), some_b(1))
        part = w.at[zat(k) * NY + y, :, COLS_B]
        for d in range(2):
            send(("by", k), part, part, y_to[d])

    def dn_y_half(k):
        arrived(("by", k), some_b(2))
        for d in range(2):
            part = w.at[zat(k) * NY + y_from[d], HALF[d], COLS_B]
            send(("byh", k), part, part, y_to[d])

    def dn_turn(k):
        arrived(("byh", k), some_b(1))
        zz = zat(k)
        slab = w[pl.ds(zz * NY, NY), :, pl.ds(HID, HID)].reshape(NY * WR, HID)
        wt[:, pl.ds(pl.multiple_of(zz * NY * WR, NY * WR), NY * WR)] = slab.T

    loads["ld"].wait()
    loads["k"].wait()
    loads["v"].wait()
    load("up", up_h, w.at[sp, :, pl.ds(0, HID)], 3)
    load("dn", dn_h, w.at[sp, :, pl.ds(HID, HID)], 4)
    load("q", q_h, q_v, 5)
    load("g", g_h, g_v, 6)
    load("ow", ow_h, ow_v, 7)
    load("stream", stream_h, stream_v, 8)
    load("hg", hg_h, hg_ref, 9)
    load("mg", mg_h, mg_ref, 10)
    r_i = lax.broadcasted_iota(jnp.int32, (256, 256), 0)
    c_i = lax.broadcasted_iota(jnp.int32, (256, 256), 1)
    tri = jnp.where((c_i > r_i) & (c_i // BLOCK == r_i // BLOCK), 1.0, 0.0).astype(BF16)

    def group(gi, state, total):
        rows = slice(gi * 256, (gi + 1) * 256)
        ld = ld_v[rows, :]
        hi, lo = _split(ld)
        lo2 = (ld - hi.astype(F32) - lo.astype(F32)).astype(BF16)
        suf = _dot(tri, hi) + _dot(tri, lo) + _dot(tri, lo2)
        dk = k_v[rows, :].astype(F32) * jnp.exp(suf)
        dk_hi, dk_lo = _split(dk)
        vals = v_v[rows, :]
        for b in range(4):
            s = slice(b * BLOCK, (b + 1) * BLOCK)
            vv = jnp.concatenate([vals[s], vals[s]], axis=0)
            dd = jnp.concatenate([dk_hi[s], dk_lo[s]], axis=0)
            upd = _dot(vv, dd, (((0,), (0,)), ((), ())))
            last = suf[b * BLOCK : b * BLOCK + 1] + ld[b * BLOCK : b * BLOCK + 1]
            state = jnp.exp(last) * state + upd
            total = total + last
            sloc[gi * 4 + b] = state
            cl[gi * 4 + b] = jnp.broadcast_to(total, (8, KC))
        return state, total

    state, total = jnp.zeros((DV, KC), F32), jnp.zeros((1, KC), F32)
    for gi in range(NB // 4):
        state, total = group(gi, state, total)

    QV = DV // NY

    def with_log(block, log):
        hi, lo = _split(log)
        lo2 = (log - hi.astype(F32) - lo.astype(F32)).astype(BF16)
        sub = lax.broadcasted_iota(jnp.int32, (16, KC), 0)
        logs = jnp.where(
            sub == 0,
            hi.astype(F32),
            jnp.where(sub == 1, lo.astype(F32), jnp.where(sub == 2, lo2.astype(F32), 0.0)),
        )
        return jnp.concatenate([block, logs], axis=0).astype(BF16)

    def block_log(tile):
        t = tile.astype(F32)
        return t[:QV], t[QV : QV + 1] + t[QV + 1 : QV + 2] + t[QV + 2 : QV + 3]

    def first(ref, count):
        return ref.at[pl.ds(0, count)]

    def scatter(name, count, src_of, dst, to):
        def one(d, carry):
            pltpu.make_async_remote_copy(
                src_ref=src_of(d),
                dst_ref=dst,
                send_sem=ssem.at[SEND[name]],
                recv_sem=rsem.at[RECV[(name,)]],
                device_id=to(d),
                device_id_type=MESH,
            ).start()
            return carry

        lax.fori_loop(1, count, one, 0)

    def y_at(d):
        return lax.rem(y + d, NY)

    for p in range(NY):
        sx_send[p] = with_log(state[p * QV : (p + 1) * QV], total)

    pl.semaphore_wait(barrier, NY - 1 + NZ - 1 + 3)
    scatter("st1", NY, lambda d: sx_send.at[y_at(d)], sx_recv.at[y], lambda d: {"sp_1": y_at(d)})
    sx_recv[y] = sx_send[y]
    loads["up"].wait()
    loads["dn"].wait()
    up_y()
    dn_y(0)
    dn_z(1)
    arrived(("st1",), first(sx_recv, NY - 1))

    group_state, group_log = block_log(sx_recv[0])
    for p in range(1, NY):
        more, log = block_log(sx_recv[p])
        group_state = jnp.exp(log) * group_state + more
        group_log = group_log + log
    zx_send[...] = with_log(group_state, group_log)
    scatter(
        "st2", NZ, lambda d: zx_send, zx_recv.at[z], lambda d: {"sp_0": lax.rem(z + d, NZ)}
    )
    zx_recv[z] = zx_send[...]
    up_y_half()
    dn_y(1)
    dn_z(2)
    arrived(("st2",), first(zx_recv, NZ - 1))

    run = jnp.zeros((QV, KC), F32)
    for e in range(NZ):
        more, log = block_log(zx_recv[e])
        run = jnp.where(e < z, jnp.exp(log) * run + more, run)
    for p in range(NY):
        px_send[p] = run.astype(BF16)
        more, log = block_log(sx_recv[p])
        run = jnp.exp(log) * run + more
    scatter("st3", NY, lambda d: px_send.at[y_at(d)], px_recv.at[y], lambda d: {"sp_1": y_at(d)})
    px_recv[y] = px_send[y]

    dn_y(7)
    dn_y_half(0)
    up_z(1, 0)
    loads["q"].wait()
    loads["g"].wait()
    loads["ow"].wait()
    loads["hg"].wait()

    def gate_rows_of(n, carry):
        rows = pl.ds(pl.multiple_of(n * 256, 256), 256)
        gate = g_v[rows, :].astype(F32)
        gate_v[rows, :] = hg_ref[...] * (gate / (1.0 + jnp.exp(-gate)))
        return carry

    lax.fori_loop(0, ROWS // 256, gate_rows_of, 0)
    dn_z(3)
    dn_y(2)
    dn_y(6)
    up_z(1, 1)
    arrived(("st3",), first(px_recv, NY - 1))

    def attend(j):
        s_in = px_recv[...].astype(F32).reshape(DV, KC)
        base = lax.rem(x + j, NX) * 4
        outs = []
        for half in range(2):
            first = base + (1 - c if half == 0 else c) * 2
            for b in range(2):
                n = first + b
                rows = pl.ds(pl.multiple_of(n * BLOCK, BLOCK), BLOCK)
                full = sloc[n] + jnp.exp(cl[n][0:1]) * s_in
                f_hi, f_lo = _split(full)
                qq = q_v[rows, :]
                read = _dot(
                    jnp.concatenate([qq, qq], axis=1),
                    jnp.concatenate([f_hi, f_lo], axis=1),
                    (((1,), (1,)), ((), ())),
                ) * (KC**-0.5)
                scaled = read * lax.rsqrt(jnp.mean(read * read, axis=-1, keepdims=True) + EPS)
                outs.append((scaled * gate_v[rows, :]).astype(BF16))
        heads = jnp.concatenate(outs, axis=0)
        for n in range(4):
            cols = slice(n * 512, (n + 1) * 512)
            part = _dot(heads, ow_v[:, cols])
            psend[0, SLOT[j], :, cols] = part[:OWN].astype(BF16)
            pown[SLOT[j], :, cols] = part[OWN:]
        for name, rows in pair_parts(j):
            send(("dd0", name), psend.at[0, SLOT[j], rows], precv.at[0, SLOT[j], rows], sib)

    def views(rs, n):
        r0, nr, c0, nc = CHUNKS[rs][n]
        return pl.ds(r0, nr), pl.ds(c0, nc), pl.ds(r0 // 2, nr // 2), nr // 2, r0

    def pair_parts(j):
        if j == 2:
            return (((2, 0), pl.ds(0, QR)), ((2, 1), pl.ds(QR, OWN - QR)))
        return ((j, pl.ds(0, OWN)),)

    def pair_sum(rs, j, n):
        rows, cols, _, _, _ = views(rs, n)
        if rs == 0:
            name, part = pair_parts(j)[1 if j == 2 and n > 0 else 0]
            arrived(("dd0", name), precv.at[0, SLOT[j], part])
        elif j == 2:
            arrived(("dd1", 0, n), precv.at[1, 0, rows, cols])
        else:
            arrived(("dd1", 1, n), precv.at[1, pl.ds(1, 3), rows, cols])
        return pown[SLOT[j], rows, cols] + precv[rs, SLOT[j], rows, cols].astype(F32)

    def ring_1(rs, n):
        rows, cols, half, h2, r0 = views(rs, n)
        cs[rs, 0, rows, cols] = pair_sum(rs, 2, n).astype(BF16)
        for d in range(2):
            send(
                (("rx", rs, 1), n),
                cs.at[rs, 0, pl.ds(r0 + d * h2, h2), cols],
                r1.at[rs, d, half, cols],
                x_to[d],
            )

    def ring_2(rs, n):
        rows, cols, half, h2, _ = views(rs, n)
        both = [pair_sum(rs, 1, n), pair_sum(rs, 3, n)]
        arrived((("rx", rs, 1), n), r1.at[rs, :, half, cols])
        for d in range(2):
            more = r1[rs, d, half, cols].astype(F32)
            if d == 0:
                total = jnp.concatenate([both[d][:h2] + more, both[d][h2:]], axis=0)
            else:
                total = jnp.concatenate([both[d][:h2], both[d][h2:] + more], axis=0)
            cs[rs, 1 + d, rows, cols] = total.astype(BF16)
            send((("rx", rs, 2), n), cs.at[rs, 1 + d, rows, cols], r2.at[rs, d, rows, cols], x_to[d])

    def ring_end(rs, n):
        rows, cols, _, _, _ = views(rs, n)
        total = pair_sum(rs, 0, n)
        arrived((("rx", rs, 2), n), r2.at[rs, :, rows, cols])
        return total + r2[rs, 0, rows, cols].astype(F32) + r2[rs, 1, rows, cols].astype(F32)

    def rows_of(q):
        return pl.ds(q * QR, QR)

    def norm_rows(q):
        rows = rows_of(q)
        mid = (stream_v[rows, :].astype(F32) + ring_end(0, q)).astype(BF16)
        mid_v[rows, :] = mid
        midf = mid.astype(F32)
        nrm[1, 0, rows, :] = (
            midf * lax.rsqrt(jnp.mean(midf * midf, axis=-1, keepdims=True) + EPS) * mg_ref[...]
        ).astype(BF16)

    def spread_rows(q):
        rows = rows_of(q)
        for d in range(2):
            send(("ag", q), nrm.at[1, 0, rows], nrm.at[1, 3 if d == 0 else 1, rows], x_to[d])
        send(("ags", q), nrm.at[1, 0, rows], nrm.at[0, 0, rows], sib)

    def spread_mid(q):
        rows = rows_of(q)
        arrived(("ag", q), nrm.at[1, pl.ds(0, 2), rows])
        for d in range(2):
            j = 3 if d == 0 else 1
            part = pl.ds(q * QR + d * (QR // 2), QR // 2)
            send(("agh", q), nrm.at[1, j, part], nrm.at[1, 2, part], x_to[d])
            send(("ags", q), nrm.at[1, j, rows], nrm.at[0, j, rows], sib)

    def spread_end(q):
        rows = rows_of(q)
        arrived(("agh", q), nrm.at[1, 2, rows])
        send(("ags", q), nrm.at[1, 2, rows], nrm.at[0, 2, rows], sib)

    def spread_done(q):
        arrived(("ags", q), nrm.at[0, :, rows_of(q)])

    def ff_up(q, half):
        x_in = nrm[:, :, rows_of(q)].reshape(8 * QR, D)
        for c0 in range(half * (HID // 2), (half + 1) * (HID // 2), 256):
            pre = _dot(x_in, w[:, :, c0 : c0 + 256].reshape(D, 256))
            pre = jnp.maximum(pre, 0.0)
            hid_v[:, c0 : c0 + 256] = (pre * pre).astype(BF16)

    def ff_down(q, g):
        n = G * q + g
        rows, cols, _, _, _ = views(1, n)
        for c0 in range(g * (D // G), (g + 1) * (D // G), 256):
            part = _dot(hid_v[...], wt[:, c0 : c0 + 256]).reshape(2, 4, QR, 256)
            for j in range(4):
                psend[1, SLOT[j], rows, c0 : c0 + 256] = part[0, j].astype(BF16)
                pown[SLOT[j], rows, c0 : c0 + 256] = part[1, j]
        for i, slots in enumerate((pl.ds(0, 1), pl.ds(1, 3))):
            send(("dd1", i, n), psend.at[1, slots, rows, cols], precv.at[1, slots, rows, cols], sib)

    def out_rows(n):
        rows, cols, _, _, _ = views(1, n)
        out_ref[rows, cols] = (mid_v[rows, cols].astype(F32) + ring_end(1, n)).astype(BF16)

    attend(2)
    attend(1)
    ring_1(0, 0)
    ring_1(0, 1)
    ring_1(0, 2)
    ring_1(0, 3)
    attend(3)
    attend(0)
    dn_y_half(1)
    dn_y_half(7)
    up_z(2, 0)
    ring_2(0, 0)
    ring_2(0, 1)
    ring_2(0, 2)
    dn_z(4)
    dn_y(3)
    dn_y(5)
    ring_2(0, 3)
    dn_y_half(2)
    dn_y_half(6)
    up_z(2, 1)
    loads["stream"].wait()
    loads["mg"].wait()
    norm_rows(0)
    spread_rows(0)
    dn_turn(0)
    norm_rows(1)
    spread_rows(1)
    up_z(3, 0)
    dn_y(4)
    norm_rows(2)
    dn_turn(1)
    dn_turn(7)
    up_z(3, 1)
    norm_rows(3)
    spread_mid(0)
    spread_rows(2)
    up_z(4, 0)
    dn_y_half(3)
    dn_y_half(5)
    spread_mid(1)
    spread_rows(3)
    dn_turn(2)
    dn_turn(6)
    spread_end(0)
    dn_y_half(4)
    up_z(4, 1)
    spread_mid(2)
    up_done()
    spread_done(0)
    ff_up(0, 0)
    dn_turn(3)
    dn_turn(5)
    spread_end(1)
    dn_turn(4)
    ff_up(0, 1)
    ff_down(0, 0)
    ff_down(0, 1)
    spread_done(1)
    ff_up(1, 0)
    spread_mid(3)
    ring_1(1, 0)
    ff_up(1, 1)
    ring_1(1, 1)
    spread_end(2)
    ff_down(1, 0)
    ff_down(1, 1)
    spread_done(2)
    ff_up(2, 0)
    ring_1(1, 2)
    ff_up(2, 1)
    ring_1(1, 3)
    spread_end(3)
    ring_2(1, 0)
    ff_down(2, 0)
    ff_down(2, 1)
    ring_2(1, 1)
    spread_done(3)
    ff_up(3, 0)
    ring_1(1, 4)
    ring_2(1, 2)
    ff_up(3, 1)
    ring_1(1, 5)
    ff_down(3, 0)
    ring_2(1, 3)
    ff_down(3, 1)
    ring_2(1, 4)
    ring_1(1, 6)
    ring_1(1, 7)
    ring_2(1, 5)
    out_rows(0)
    ring_2(1, 6)
    ring_2(1, 7)
    out_rows(1)
    out_rows(2)
    out_rows(3)
    out_rows(4)
    out_rows(5)
    out_rows(6)
    out_rows(7)

    for family, size in (
        ("az", some_a(31)),
        ("bz", some_b(31)),
        ("st1", first(sx_send, NY - 1)),
        ("st2", first(zx_recv, NZ - 1)),
        ("st3", first(px_send, NY - 1)),
        ("dd0", psend),
        ("rx", cs),
        ("ag", nrm.at[1, pl.ds(0, 2)]),
        ("agh", nrm.at[1, 0]),
        ("ags", nrm.at[0]),
    ):
        sent(family, size)


def local(
    stream,
    query_rows,
    key_rows,
    value_rows,
    gate_rows,
    log_decay,
    head_gain,
    out_weight,
    mix_gain,
    up_weight,
    down_weight,
):
    any_spec = pl.BlockSpec(memory_space=pl.ANY)
    vmem = pl.BlockSpec(memory_space=pltpu.VMEM)
    return pl.pallas_call(
        kernel,
        out_shape=pltpu.VMEM((OWN, D), BF16),
        in_specs=[any_spec] * 11,
        out_specs=vmem,
        scratch_shapes=[
            pltpu.VMEM((1, DV), F32),
            pltpu.VMEM((1, D), F32),
            pltpu.VMEM((OWN, D), BF16),
            pltpu.VMEM((ROWS, KC), BF16),
            pltpu.VMEM((ROWS, KC), BF16),
            pltpu.VMEM((ROWS, DV), BF16),
            pltpu.VMEM((ROWS, DV), BF16),
            pltpu.VMEM((ROWS, DV), F32),
            pltpu.VMEM((ROWS, KC), F32),
            pltpu.VMEM((DV, D), BF16),
            pltpu.VMEM((NSP, WR, 2 * HID), BF16),
            pltpu.VMEM((HID, D), BF16),
            pltpu.VMEM((NB, DV, KC), F32),
            pltpu.VMEM((NB, 8, KC), F32),
            pltpu.VMEM((NY, DV // NY + 16, KC), BF16),
            pltpu.VMEM((NY, DV // NY + 16, KC), BF16),
            pltpu.VMEM((DV // NY + 16, KC), BF16),
            pltpu.VMEM((NZ, DV // NY + 16, KC), BF16),
            pltpu.VMEM((NY, DV // NY, KC), BF16),
            pltpu.VMEM((NY, DV // NY, KC), BF16),
            pltpu.VMEM((2, 4, OWN, D), BF16),
            pltpu.VMEM((2, 4, OWN, D), BF16),
            pltpu.VMEM((4, OWN, D), F32),
            pltpu.VMEM((2, 3, OWN, D), BF16),
            pltpu.VMEM((2, 2, OWN // 2, D), BF16),
            pltpu.VMEM((2, 2, OWN, D), BF16),
            pltpu.VMEM((2, 4, OWN, D), BF16),
            pltpu.VMEM((OWN, D), BF16),
            pltpu.VMEM((8 * QR, HID), BF16),
            pltpu.SemaphoreType.DMA((11,)),
            pltpu.SemaphoreType.DMA((len(SEND),)),
            pltpu.SemaphoreType.DMA((len(RECV),)),
        ],
        compiler_params=pltpu.CompilerParams(
            collective_id=0, has_side_effects=True, vmem_limit_bytes=60 * 1024 * 1024
        ),
        name="layer",
    )(
        stream,
        query_rows,
        key_rows,
        value_rows,
        gate_rows,
        log_decay,
        head_gain.reshape(1, DV),
        out_weight,
        mix_gain.reshape(1, D),
        up_weight,
        down_weight,
    )


def solution(mesh):
    torus = Mesh(mesh.devices.reshape(NZ, NY, NX, 2), SP_TP)
    in_specs = (
        P(SP_TP, None),
        P(SP, TP),
        P(SP, TP),
        P(SP, TP),
        P(SP, TP),
        P(SP, TP),
        P(),
        P(TP, None),
        P(),
        P(SP, TP),
        P(SP, TP),
    )
    out_specs = P(SP_TP, None)
    return jax.shard_map(local, mesh=torus, in_specs=in_specs, out_specs=out_specs, check_vma=False)
```
